32 devices in a mesh: sp: 8 (over z, x), tp: 4 (over y, core).
Axes of the slice: x: 2, y: 2, z: 4, core: 2. Of those that a mesh axis runs over, the one named last changes fastest.
Arguments:
- lane_source_signal: bfloat16 [1024, 1024], P('tp', 'sp'), may hold values from -6 to 6
- spectral_damping_part: float32 [64, 64], P('tp'), may hold values from -3 to -0.0002
- spectral_angular_part: float32 [64, 64], P('tp'), may hold values from 0.31 to 201.0624
- interval_exponent: float32 [64], P('tp'), may hold values from -3.9 to -1.6
- entry_matrix_inphase: float32 [64, 64, 16], P('tp'), may hold values from -1 to 1
- entry_matrix_quadrature: float32 [64, 64, 16], P('tp'), may hold values from -1 to 1
- emission_inphase: float32 [64, 16, 64], P('tp'), may hold values from -0.75 to 0.75
- emission_quadrature: float32 [64, 16, 64], P('tp'), may hold values from -0.75 to 0.75
- lane_bypass_factor: float32 [1024], P('tp'), may hold values from -5 to 5
- spike_shrink_offset: float32 [64, 1024], P('tp', 'sp'), may hold values from -1.4 to 0
- lane_exit_matrix: bfloat16 [1024, 4096], P('tp'), may hold values from -0.1875 to 0.1875
- skipline_stream: bfloat16 [1024, 4096], P('sp'), may hold values from -6 to 6
- specialist_scaling_vector: float32 [4096], replicated, may hold values from 0.1 to 1.9
- selected_specialists: int32 [1024, 2], P('sp'), may hold values from 0 to 7, all different within a row; in each aligned block of 128 rows (0 to 127, 128 to 255, ...) at most 64 rows name the same one
- dispatcher_scores: float32 [1024, 2], P('sp'), may hold values from 0.1 to 1
- specialist_valve_matrix: bfloat16 [8, 4096, 2048], P('sp', None, 'tp'), may hold values from -0.09375 to 0.09375
- specialist_widen_matrix: bfloat16 [8, 4096, 2048], P('sp', None, 'tp'), may hold values from -0.09375 to 0.09375
- specialist_shrink_matrix: bfloat16 [8, 2048, 4096], P('sp', 'tp'), may hold values from -0.1875 to 0.1875
Outputs:
- updated: bfloat16 [1024, 4096], P('sp', 'tp')
The draws below stay inside these ranges and needn't reach their ends.
Inputs may be any that keep to these rules, and one draw needn't show every extreme that they name: `selected_specialists`: each row names 2 different experts. Among the rows of each aligned block of 128 positions no expert is named more than 64 times, and in every block some expert is named exactly 64 times.
All inputs are finite; a program needn't handle non-finite values.
Results may differ from the reference program's by a relative error of at most 0.019.
Values may be sent and summed in bfloat16 or wider, within the bound.
A program may use at most 64 MiB of HBM per device.

```python
import math
import jax
import jax.numpy as jnp
import numpy as np
from jax import lax

D = 4096
C = 1024
GS = 16
P_SIZE = 64
F = 2048
TOPK = 2
TOK_DEV = 128
G = 64
TOKENS = 1024
EXPERTS = 8
CAP = 64
N_SP = 8
N_TP = 4


def draw_spectral_damping_part(key, part):
    subkeys = jax.random.split(key, 3)
    fast_group = jax.random.uniform(subkeys[0], (G, 1)) < 0.5
    quick_rate = -jax.random.uniform(subkeys[1], (G, P_SIZE), jnp.float32, 1.0, 3.0)
    slow_rate = -jnp.exp(jax.random.uniform(subkeys[2], (G, P_SIZE), jnp.float32, math.log(0.0002), math.log(0.001)))
    return jnp.where(fast_group, quick_rate, slow_rate)


def draw_spectral_angular_part(key, part):
    offset = jax.random.uniform(key, (G, P_SIZE), jnp.float32, 0.1, 0.9)
    return math.pi * (jnp.arange(P_SIZE, dtype=jnp.float32)[None, :] + offset)


def draw_spike_shrink_offset(key, part):
    subkeys = jax.random.split(key, 3)
    blocks = TOKENS // 32
    block_rate = jnp.exp(jax.random.uniform(subkeys[0], (G, blocks), jnp.float32, math.log(2.5e-05), math.log(0.0001)))
    baseline = -jnp.repeat(block_rate, 32, axis=1)
    spots = jax.random.randint(subkeys[1], (G, 2), 0, TOKENS)
    losses = jnp.log(1.0 - jax.random.uniform(subkeys[2], (G, 2), jnp.float32, 0.2, 0.5))
    position = jnp.arange(TOKENS, dtype=jnp.int32)[None, :, None]
    struck = position == spots[:, None, :]
    return baseline + jnp.sum(jnp.where(struck, losses[:, None, :], 0.0), axis=2)


def raised(result, stream_key, source, target, shards_of, factor):
    owner, partner = [(jnp.arange(result.shape[dim]) // (result.shape[dim] // shards_of)).reshape([-1 if axis == dim else 1 for axis in range(result.ndim)]) for dim in (source, target)]
    chosen = jax.random.permutation(stream_key, shards_of)[partner]
    strong = (owner == chosen) | (owner == (partner + shards_of // 2) % shards_of)
    return jnp.where(strong, factor * result, result)


def steps_of(stream_key, shape, cuts, smallest, top_value):
    def one(dim, shards_of):
        steps = jax.random.uniform(jax.random.fold_in(jax.random.fold_in(stream_key, 6), dim), (shards_of,), jnp.float32, smallest / len(cuts), top_value / len(cuts))
        return jnp.repeat(jnp.exp(steps), shape[dim] // shards_of).reshape((-1,) + (1,) * (len(shape) - dim - 1))

    factor_of = one(*cuts[0])
    for cut in cuts[1:]:
        factor_of = factor_of * one(*cut)
    return factor_of


def assign_block(rng, own, number, rows, number_of, top, most, skew):
    sequence = jax.random.permutation(rng, number_of)
    crowded, common = shares(number_of, rows * top, most, skew, True), shares(number_of, rows * top, most, skew, False)
    places = jnp.arange(number_of)

    def named(tallies, turn):
        used = int((tallies > 0).sum())
        fixed = max(1, used // 4)
        moved = fixed + (places - fixed + turn * (used - fixed)) % max(1, number_of - fixed)
        return jnp.zeros((number_of,), jnp.int32).at[sequence[jnp.where(places < fixed, places, moved)]].set(jnp.asarray(tallies, jnp.int32))

    tallies = jnp.where(number % 4 == 0, named(crowded, number // 4), named(common, number - number // 4 - 1))
    mixed = jax.random.permutation(jax.random.fold_in(own, 3), number_of)
    giver, sink = mixed[0:number_of // 2 * 2:2], mixed[1:number_of // 2 * 2:2]
    slack = jnp.minimum(tallies[giver] - 1, most - tallies[sink]) // 2
    slack = jnp.where((giver == sequence[0]) | (sink == sequence[0]) | (tallies[sink] == 0), 0, jnp.maximum(slack, 0))
    moved = jax.random.randint(jax.random.fold_in(own, 4), (number_of // 2,), 0, 1 << 20) % (slack + 1)
    tallies = tallies.at[giver].add(-moved).at[sink].add(moved)
    members = jnp.searchsorted(jnp.cumsum(tallies), jnp.arange(rows * top), side="right").astype(jnp.int32)
    listing = members.reshape(top, rows).T
    listing = listing[jax.random.permutation(jax.random.fold_in(own, 1), rows)]
    turn = jax.random.randint(jax.random.fold_in(own, 2), (rows, 1), 0, top)
    return jnp.take_along_axis(listing, (jnp.arange(top)[None, :] + turn) % top, axis=1)


def shares(number_of, total, reach, lean, full):
    loads = [(1 << 20) // math.isqrt(grade ** lean) + 1 for grade in range(1, number_of + 1)]
    largest = reach if full else min(reach, max(-(-total // number_of), total * loads[0] // sum(loads)))
    least = 1 if total - largest >= number_of - 1 else 0
    given, surplus = [largest] + [least] * (number_of - 1), total - largest - least * (number_of - 1)
    while surplus > 0:
        free = [i for i in range(1, number_of) if given[i] < largest] or [i for i in range(1, number_of) if given[i] < reach]
        whole, left = sum([loads[i] for i in free]), surplus
        for i in free:
            more = min(reach - given[i], max(1, left * loads[i] // whole), surplus)
            given[i] = given[i] + more
            surplus = surplus - more
    return np.array(given)


def centred(key, shape, width, most, pieces=(), kind=jnp.bfloat16):
    gain = steps_of(key, shape, pieces, -0.22, 0.18) if pieces else 1.0
    result = jax.random.normal(key, shape, jnp.float32) * width * gain
    return jnp.minimum(jnp.maximum(result, -most), most).astype(kind)


def heavy_noise(own_key, extent, width, most, shards, heavy, kind=jnp.bfloat16):
    array = width * jax.random.normal(own_key, extent, jnp.float32)
    if shards:
        array = array * steps_of(own_key, extent, shards, -0.22, 0.18)
    return jnp.clip(raised(array, jax.random.fold_in(own_key, 3), *heavy), -most, most).astype(kind)


def setup_inputs(seed: int = 0) -> dict:
    streams_of = jax.random.split(jax.random.key(seed), 19)
    lane_source_signal = centred(streams_of[0], (C, TOKENS), 1.0, 6.0, ((0, 4), (1, 8)))
    spectral_damping_part = draw_spectral_damping_part(jax.random.fold_in(streams_of[18], 71), 0)
    spectral_angular_part = draw_spectral_angular_part(jax.random.fold_in(streams_of[18], 71), 0)
    interval_exponent = jnp.clip(-3.9 + 2.3000001 * jax.random.uniform(streams_of[3], (G,), jnp.float32) ** steps_of(streams_of[3], (G,), ((0, 4),), -0.2, 0.2), -3.9, -1.6)
    entry_matrix_inphase = centred(streams_of[4], (G, P_SIZE, GS), (2 * GS) ** -0.5, 1.0, ((0, 4),), jnp.float32)
    entry_matrix_quadrature = centred(streams_of[5], (G, P_SIZE, GS), (2 * GS) ** -0.5, 1.0, ((0, 4),), jnp.float32)
    emission_inphase = centred(streams_of[6], (G, GS, P_SIZE), P_SIZE ** -0.5, 0.75, ((0, 4),), jnp.float32)
    emission_quadrature = centred(streams_of[7], (G, GS, P_SIZE), P_SIZE ** -0.5, 0.75, ((0, 4),), jnp.float32)
    lane_bypass_factor = centred(streams_of[8], (C,), 1.0, 5.0, ((0, 4),), jnp.float32)
    spike_shrink_offset = draw_spike_shrink_offset(jax.random.fold_in(streams_of[18], 71), 0)
    lane_exit_matrix = centred(streams_of[10], (C, D), C ** -0.5, 0.1875, ((0, 4),))
    skipline_stream = centred(streams_of[11], (TOKENS, D), 1.0, 6.0, ((0, 8),))
    specialist_scaling_vector = jnp.clip(1.0 + 0.18 * jax.random.normal(streams_of[12], (D,), jnp.float32), 0.1, 1.9)
    selected_specialists_keys = jax.random.split(jax.random.fold_in(streams_of[13], 1), TOKENS // TOK_DEV)
    selected_specialists_turns = jax.random.permutation(jax.random.fold_in(streams_of[13], 3), TOKENS // TOK_DEV)
    selected_specialists = jax.vmap(lambda own, number: assign_block(jax.random.fold_in(streams_of[13], 2), own, number, TOK_DEV, EXPERTS, TOPK, CAP, 2))(selected_specialists_keys, selected_specialists_turns).reshape((TOKENS, TOPK))
    dispatcher_scores = jnp.clip(jnp.exp(math.log(1.0) - 2.3025851 * jax.random.uniform(streams_of[14], (TOKENS, TOPK), jnp.float32) ** steps_of(streams_of[14], (TOKENS, TOPK), ((0, 8),), -0.2, 0.2)), 0.1, 1.0)
    specialist_valve_matrix = centred(streams_of[15], (EXPERTS, D, F), D ** -0.5, 0.09375, ((0, 8), (2, 4)))
    specialist_widen_matrix = centred(streams_of[16], (EXPERTS, D, F), D ** -0.5, 0.09375, ((0, 8), (2, 4)))
    specialist_shrink_matrix = heavy_noise(streams_of[17], (EXPERTS, F, D), F ** -0.5, 0.1875, ((0, 8), (1, 4)), (1, 2, 4, 2.0))
    return {"lane_source_signal": lane_source_signal, "spectral_damping_part": spectral_damping_part, "spectral_angular_part": spectral_angular_part, "interval_exponent": interval_exponent, "entry_matrix_inphase": entry_matrix_inphase, "entry_matrix_quadrature": entry_matrix_quadrature, "emission_inphase": emission_inphase, "emission_quadrature": emission_quadrature, "lane_bypass_factor": lane_bypass_factor, "spike_shrink_offset": spike_shrink_offset, "lane_exit_matrix": lane_exit_matrix, "skipline_stream": skipline_stream, "specialist_scaling_vector": specialist_scaling_vector, "selected_specialists": selected_specialists, "dispatcher_scores": dispatcher_scores, "specialist_valve_matrix": specialist_valve_matrix, "specialist_widen_matrix": specialist_widen_matrix, "specialist_shrink_matrix": specialist_shrink_matrix}


EPS = 1e-06
PRECISE_MODE = lax.Precision.HIGHEST

def affine_pair(earlier, latter):
    mul_re = earlier[0] * latter[0] - earlier[1] * latter[1]
    mul_im = earlier[0] * latter[1] + earlier[1] * latter[0]
    add_re = latter[0] * earlier[2] - latter[1] * earlier[3] + latter[2]
    add_im = latter[0] * earlier[3] + latter[1] * earlier[2] + latter[3]
    return (mul_re, mul_im, add_re, add_im)

def bundled_recurrence_layer(packed):
    u_group, a_real, a_imag, log_dt, b_real, b_imag, c_real, c_imag, skip_group, extra_row = packed
    step_size = jnp.exp(log_dt)
    natural_pace_exponent = a_real * step_size
    angle = a_imag * step_size
    num_re = jnp.expm1(natural_pace_exponent) * jnp.cos(angle) - 2.0 * jnp.sin(0.5 * angle) ** 2
    num_im = jnp.exp(natural_pace_exponent) * jnp.sin(angle)
    denom = a_real * a_real + a_imag * a_imag
    fac_re = (num_re * a_real + num_im * a_imag) / denom
    fac_im = (num_im * a_real - num_re * a_imag) / denom
    map_re = fac_re[:, None] * b_real - fac_im[:, None] * b_imag
    map_im = fac_re[:, None] * b_imag + fac_im[:, None] * b_real
    drive_re = jnp.dot(map_re, u_group, precision=PRECISE_MODE)
    drive_im = jnp.dot(map_im, u_group, precision=PRECISE_MODE)
    recurrence_modulus = jnp.exp(natural_pace_exponent[:, None] + extra_row[None, :])
    trans_re = recurrence_modulus * jnp.cos(angle)[:, None]
    trans_im = recurrence_modulus * jnp.sin(angle)[:, None]
    scanned = lax.associative_scan(affine_pair, (trans_re, trans_im, drive_re, drive_im), axis=1)
    value = jnp.dot(c_real, scanned[2], precision=PRECISE_MODE) - jnp.dot(c_imag, scanned[3], precision=PRECISE_MODE) + skip_group[:, None] * u_group
    return jax.nn.gelu(value).astype(jnp.bfloat16)

def reference(lane_source_signal, spectral_damping_part, spectral_angular_part, interval_exponent, entry_matrix_inphase, entry_matrix_quadrature, emission_inphase, emission_quadrature, lane_bypass_factor, spike_shrink_offset, lane_exit_matrix, skipline_stream, specialist_scaling_vector, selected_specialists, dispatcher_scores, specialist_valve_matrix, specialist_widen_matrix, specialist_shrink_matrix):
    f32 = jnp.float32
    bf16 = jnp.bfloat16
    bundle_total = spectral_damping_part.shape[0]
    lanes_within_bundle = entry_matrix_inphase.shape[2]
    length = lane_source_signal.shape[1]
    bundled_signal = lane_source_signal.astype(f32).reshape(bundle_total, lanes_within_bundle, length)
    recurrence_result = lax.map(bundled_recurrence_layer, (bundled_signal, spectral_damping_part, spectral_angular_part, interval_exponent, entry_matrix_inphase, entry_matrix_quadrature, emission_inphase, emission_quadrature, lane_bypass_factor.reshape(bundle_total, lanes_within_bundle), spike_shrink_offset))
    recurrence_result = recurrence_result.reshape(bundle_total * lanes_within_bundle, length)
    projected = jnp.dot(recurrence_result.T, lane_exit_matrix, preferred_element_type=f32).astype(bf16)
    stream = (skipline_stream.astype(f32) + lax.optimization_barrier(projected).astype(f32)).astype(bf16)
    stream_f = lax.optimization_barrier(stream).astype(f32)
    inv_rms = lax.rsqrt(lax.optimization_barrier(jnp.mean(stream_f * stream_f, axis=-1, keepdims=True)) + EPS)
    normed = (stream_f * inv_rms * specialist_scaling_vector).astype(bf16)
    share = dispatcher_scores / lax.optimization_barrier(jnp.sum(dispatcher_scores, axis=1, keepdims=True))
    flat_routes = selected_specialists.reshape(-1)
    flat_share = share.reshape(-1)
    slots = N_SP * CAP
    block_units = F // N_TP

    def one_expert(total, packed):
        gate_w, up_w, down_w, expert_id = packed
        chosen = flat_routes == expert_id
        positions = jnp.nonzero(chosen, size=slots, fill_value=0)[0].astype(jnp.int32)
        valid = jnp.arange(slots, dtype=jnp.int32) < jnp.sum(chosen.astype(jnp.int32))
        token_ids = positions // TOPK
        rows = normed[token_ids]
        gate_part = jnp.dot(rows, gate_w, preferred_element_type=f32)
        up_part = jnp.dot(rows, up_w, preferred_element_type=f32)
        hidden = (jax.nn.silu(gate_part) * up_part).astype(bf16)
        hidden_blocks = jnp.transpose(hidden.reshape(slots, N_TP, block_units), (1, 0, 2))
        down_blocks = down_w.reshape(N_TP, block_units, down_w.shape[1])

        def add_block(acc, pair):
            part = jnp.dot(pair[0], pair[1], preferred_element_type=f32).astype(bf16)
            return (acc + lax.optimization_barrier(part).astype(f32), None)
        acc0 = jnp.zeros((slots, down_w.shape[1]), f32)
        summed, _ = lax.scan(add_block, acc0, (hidden_blocks, down_blocks))
        expert_out = lax.optimization_barrier(summed.astype(bf16)).astype(f32)
        weights = jnp.where(valid, flat_share[positions], 0.0)
        return (total.at[token_ids].add(weights[:, None] * expert_out), None)
    start = jnp.zeros(stream_f.shape, f32)
    experts = specialist_valve_matrix.shape[0]
    moe, _ = lax.scan(one_expert, start, (specialist_valve_matrix, specialist_widen_matrix, specialist_shrink_matrix, jnp.arange(experts, dtype=jnp.int32)))
    return (stream_f + moe).astype(bf16)
```

```python
import jax
import jax.numpy as jnp
from jax import lax
from jax.experimental import pallas as pl
from jax.experimental.pallas import tpu as pltpu
from jax.sharding import PartitionSpec as P

EPS = 1e-06


MESH = pl.DeviceIdType.MESH
VM = pl.BlockSpec(memory_space=pltpu.VMEM)
DMA = pltpu.SemaphoreType.DMA
VMEM_ROOM = 48 * 1024 * 1024


def greet(peers):
    barrier = pltpu.get_barrier_semaphore()
    for peer in peers:
        pl.semaphore_signal(barrier, inc=1, device_id=peer, device_id_type=MESH)
    pl.semaphore_wait(barrier, len(peers))


def remote(src, dst, send, recv, where):
    return pltpu.make_async_remote_copy(
        src_ref=src, dst_ref=dst, send_sem=send, recv_sem=recv, device_id=where, device_id_type=MESH
    )


def places():
    n_sp, n_tp = lax.axis_size("sp"), lax.axis_size("tp")
    return n_sp, n_tp, lax.axis_index("sp"), lax.axis_index("tp")


def tp_peers(n_tp, me, lane):
    return [(me, lax.rem(lane + i, n_tp)) for i in range(1, n_tp)]


def sp_peers(n_sp, me, lane):
    return [(lax.rem(me + i, n_sp), lane) for i in range(1, n_sp)]


def affine_pair(earlier, latter):
    mul_re = earlier[0] * latter[0] - earlier[1] * latter[1]
    mul_im = earlier[0] * latter[1] + earlier[1] * latter[0]
    add_re = latter[0] * earlier[2] - latter[1] * earlier[3] + latter[2]
    add_im = latter[0] * earlier[3] + latter[1] * earlier[2] + latter[3]
    return (mul_re, mul_im, add_re, add_im)


def dot_nt(a, b, precision=None):
    return lax.dot_general(
        a, b, (((1,), (1,)), ((), ())), precision=precision, preferred_element_type=jnp.float32
    )


def iota(shape, dim):
    return lax.broadcasted_iota(jnp.int32, shape, dim)


def expm1_of(x):
    series = jnp.ones_like(x)
    for k in range(11, 1, -1):
        series = 1.0 + x * series * (1.0 / k)
    return jnp.where(jnp.abs(x) < 0.7, x * series, jnp.exp(x) - 1.0)


def mixer_kernel(
    u, damp, ang, log_dt, ent_re, ent_im, emi_re, emi_im, bypass, shrink, sel, scores,
    rows_out, hot_out, pick_out, share_out,
    xr, xi, cr, ci, mine, pieces, send, recv,
):
    f32, bf16 = jnp.float32, jnp.bfloat16
    n_sp, n_tp, me, lane = places()
    barrier = pltpu.get_barrier_semaphore()
    for peer in sp_peers(n_sp, me, lane):
        pl.semaphore_signal(barrier, inc=1, device_id=peer, device_id_type=MESH)

    groups, p_size = damp.shape
    chans, tok = u.shape
    gs = chans // groups
    states = groups * p_size
    tiles = states // 128
    per = 128 // p_size
    n_j = 8
    n_i = tok // n_j

    def lane_group(rows):
        return iota((rows, 128), 1) // p_size

    def as_row(a):
        wide = jnp.concatenate([a] * per, axis=1)
        parts = []
        for tile in range(tiles):
            row = wide[per * tile : per * tile + 1]
            for k in range(1, per):
                row = jnp.where(lane_group(1) == k, wide[per * tile + k : per * tile + k + 1], row)
            parts.append(row)
        return jnp.concatenate(parts, axis=1)

    def spread(columns, tile):
        out = jnp.broadcast_to(columns[:, per * tile : per * tile + 1], (tok, 128))
        for k in range(1, per):
            other = jnp.broadcast_to(columns[:, per * tile + k : per * tile + k + 1], (tok, 128))
            out = jnp.where(lane_group(tok) == k, other, out)
        return out

    eye = (iota((groups, groups), 0) == iota((groups, groups), 1)).astype(f32)
    dt = jnp.exp(jnp.sum(eye * log_dt[...], axis=1, keepdims=True))
    a_re, a_im = damp[...], ang[...]
    log_rate = a_re * dt
    angle = a_im * dt
    cos, sin = jnp.cos(angle), jnp.sin(angle)
    half = jnp.sin(0.5 * angle)
    decay = jnp.exp(log_rate)
    num_re = expm1_of(log_rate) * cos - 2.0 * half * half
    num_im = decay * sin
    denom = a_re * a_re + a_im * a_im
    fac_re = as_row((num_re * a_re + num_im * a_im) / denom)
    fac_im = as_row((num_im * a_re - num_re * a_im) / denom)
    lam_re = as_row(decay * cos)
    lam_im = as_row(decay * sin)

    order = iota((tok, tok), 0)
    perm = ((order % n_j) * n_i + order // n_j == iota((tok, tok), 1)).astype(f32)
    columns = jnp.exp(dot_nt(perm, shrink[...], lax.Precision.HIGHEST))
    signal = dot_nt(perm.astype(bf16), u[...])
    eye_c = (iota((gs, gs), 0) == iota((gs, gs), 1)).astype(f32)
    in_re = dot_nt(eye_c, ent_re[...], lax.Precision.HIGHEST)
    in_im = dot_nt(eye_c, ent_im[...], lax.Precision.HIGHEST)
    same = iota((chans, states), 0) // gs == iota((chans, states), 1) // p_size

    def block_rows(a):
        return jnp.where(same, jnp.concatenate([a] * groups, axis=0), 0.0)

    drive_re = jnp.dot(
        signal, block_rows(fac_re * in_re - fac_im * in_im),
        precision=lax.Precision.HIGH, preferred_element_type=f32,
    )
    drive_im = jnp.dot(
        signal, block_rows(fac_re * in_im + fac_im * in_re),
        precision=lax.Precision.HIGH, preferred_element_type=f32,
    )
    row_j = iota((n_j, 128), 0)
    ends = []
    for tile in range(tiles):
        at = slice(128 * tile, 128 * tile + 128)
        modulus = spread(columns, tile)
        t_re, t_im = modulus * lam_re[:, at], modulus * lam_im[:, at]
        for i in range(n_i):
            step = slice(n_j * i, n_j * i + n_j)
            now = (t_re[step], t_im[step], drive_re[step, at], drive_im[step, at])
            run = now if i == 0 else affine_pair(run, now)
            for ref, value in zip((cr, ci, xr, xi), run):
                ref[step, at] = value
        off = 1
        while off < n_j:
            before = [pltpu.roll(value, off, 0) for value in run]
            joined = affine_pair(before, run)
            run = tuple(jnp.where(row_j >= off, new, old) for new, old in zip(joined, run))
            off *= 2
        for plane in range(4):
            mine[plane, tile : tile + 1, :] = run[plane][n_j - 1 : n_j]
        fills = (1.0, 0.0, 0.0, 0.0)
        ends.append(
            [jnp.where(row_j >= 1, pltpu.roll(v, 1, 0), fill) for v, fill in zip(run, fills)]
        )

    pl.semaphore_wait(barrier, n_sp - 1)

    def carry_copy(i):
        return remote(
            mine, pieces.at[i - 1], send.at[i - 1], recv.at[i - 1], (lax.rem(me + i, n_sp), lane)
        )

    for i in range(1, n_sp):
        @pl.when(me + i < n_sp)
        def _(i=i):
            carry_copy(i).start()

    share_out[...] = scores[...] / jnp.sum(scores[...], axis=1, keepdims=True)
    top = sel.shape[1]
    slots = hot_out.shape[0]
    cap = slots // n_sp
    choice = [sel[:, k : k + 1] == iota((tok, 128), 1) for k in range(top)]
    member = choice[0]
    for other in choice[1:]:
        member = member | other
    member = jnp.where(member, 1.0, 0.0)
    below = jnp.where(iota((tok, tok), 1) <= iota((tok, tok), 0), 1.0, 0.0).astype(bf16)
    rank = jnp.dot(below, member.astype(bf16), preferred_element_type=f32)
    of_slot = jnp.where(iota((slots, 128), 0) // cap == iota((slots, 128), 1), 1.0, 0.0).astype(bf16)
    code = (member * rank).astype(bf16)
    want = (iota((slots, tok), 0) % cap + 1).astype(f32)
    hot_out[...] = jnp.where(dot_nt(of_slot, code) == want, 1.0, 0.0).astype(bf16)
    want = (iota((tok, slots), 1) % cap + 1).astype(f32)
    for k in range(top):
        mark = jnp.where(choice[k], rank, 0.0).astype(bf16)
        pick_out[k] = jnp.where(dot_nt(mark, of_slot) == want, 1.0, 0.0).astype(bf16)

    out_lane = iota((chans, states), 1) // p_size
    out_row = iota((chans, states), 0) // gs

    def block_cols(a):
        wide = jnp.concatenate([a] * per, axis=1)
        return jnp.where(out_row == out_lane, jnp.concatenate([wide] * tiles, axis=1), 0.0)

    q_re, q_im = block_cols(emi_re[...]), block_cols(emi_im[...])

    for i in range(1, n_sp):
        @pl.when(me >= i)
        def _(i=i):
            carry_copy(i).wait_recv()
    run_re = jnp.zeros(mine.shape[1:], f32)
    run_im = run_re
    for i in range(n_sp - 1, 0, -1):
        mul_re, mul_im, add_re, add_im = (pieces[i - 1, plane] for plane in range(4))
        new_re = mul_re * run_re - mul_im * run_im + add_re
        new_im = mul_re * run_im + mul_im * run_re + add_im
        run_re = jnp.where(me >= i, new_re, run_re)
        run_im = jnp.where(me >= i, new_im, run_im)

    for tile in range(tiles):
        at = slice(128 * tile, 128 * tile + 128)
        p_re, p_im, z_re, z_im = ends[tile]
        e_re, e_im = run_re[tile : tile + 1], run_im[tile : tile + 1]
        z_re = z_re + p_re * e_re - p_im * e_im
        z_im = z_im + p_re * e_im + p_im * e_re
        for i in range(n_i):
            step = slice(n_j * i, n_j * i + n_j)
            c_re, c_im = cr[step, at], ci[step, at]
            xr[step, at] = xr[step, at] + c_re * z_re - c_im * z_im
            xi[step, at] = xi[step, at] + c_re * z_im + c_im * z_re
    value = (
        dot_nt(xr[...], q_re, lax.Precision.HIGH)
        - dot_nt(xi[...], q_im, lax.Precision.HIGH)
        + signal * bypass[...]
    )
    mixed = jax.nn.gelu(value).astype(bf16)
    order = iota((tok, tok), 1)
    back = ((order % n_j) * n_i + order // n_j == iota((tok, tok), 0)).astype(bf16)
    rows_out[...] = jnp.dot(back, mixed, preferred_element_type=f32).astype(bf16)

    for i in range(1, n_sp):
        @pl.when(me + i < n_sp)
        def _(i=i):
            carry_copy(i).wait_send()


def mixer_call(u, damp, ang, log_dt, ent_re, ent_im, emi_re, emi_im, bypass, shrink, sel, scores):
    n_sp = lax.axis_size("sp")
    f32, bf16 = jnp.float32, jnp.bfloat16
    chans, tok = u.shape
    groups, p_size = damp.shape
    states = groups * p_size
    top = sel.shape[1]
    slots = 2 * tok * top
    plane = (4, states // 128, 128)
    return pl.pallas_call(
        mixer_kernel,
        out_shape=(
            jax.ShapeDtypeStruct((tok, chans), bf16),
            jax.ShapeDtypeStruct((slots, tok), bf16),
            jax.ShapeDtypeStruct((top, tok, slots), bf16),
            jax.ShapeDtypeStruct((tok, top), f32),
        ),
        in_specs=[VM] * 12,
        out_specs=(VM,) * 4,
        scratch_shapes=[pltpu.VMEM((tok, states), f32)] * 4
        + [
            pltpu.VMEM(plane, f32),
            pltpu.VMEM((n_sp - 1,) + plane, f32),
            DMA((n_sp - 1,)),
            DMA((n_sp - 1,)),
        ],
        compiler_params=pltpu.CompilerParams(
            collective_id=0, has_side_effects=True, vmem_limit_bytes=VMEM_ROOM // 2
        ),
        name="mixer",
    )(u, damp, ang, log_dt, ent_re, ent_im, emi_re, emi_im, bypass, shrink, sel, scores)


def dispatch_kernel(
    rows, w, skip, gain, hot,
    stream_out, xs,
    psend, precv, ysend, yrecv, ssend, srecv, dsend,
    ps, pr, ys, yr, ss, sr, ds, dr, fs, fr, qs, qr,
):
    f32, bf16 = jnp.float32, jnp.bfloat16
    n_sp, n_tp, me, lane = places()
    n_y = n_tp // 2
    y, core = lane // 2, lax.rem(lane, 2)
    partner = (me, y * 2 + 1 - core)
    d_local = stream_out.shape[1]
    cap = hot.shape[0] // n_sp
    greet(tp_peers(n_tp, me, lane) + sp_peers(n_sp, me, lane))

    def cols(block):
        return pl.ds(pl.multiple_of(block * d_local, 128), d_local)

    def rows_of(source):
        return pl.ds(pl.multiple_of(source * cap, 16), cap)

    def part(block):
        return jnp.dot(rows[...], w[:, cols(block)], preferred_element_type=f32)

    def y_at(i):
        return lax.rem(y + i, n_y)

    waits = []

    def go(copy):
        copy.start()
        waits.append(copy)
        return copy

    pair = []
    for i in range(n_y - 1, -1, -1):
        psend[i] = part(y_at(i) * 2 + 1 - core).astype(bf16)
        pair.append(go(remote(psend.at[i], precv.at[i], ps.at[i], pr.at[i], partner)))
    pair = pair[::-1]
    across = []
    for i in range(n_y - 1, 0, -1):
        own = part(y_at(i) * 2 + core)
        pair[i].wait_recv()
        ysend[i - 1] = (own + precv[i].astype(f32)).astype(bf16)
        across.append(
            go(
                remote(
                    ysend.at[i - 1], yrecv.at[i - 1], ys.at[i - 1], yr.at[i - 1],
                    (me, y_at(i) * 2 + core),
                )
            )
        )
    total = part(lane)
    pair[0].wait_recv()
    total = total + precv[0].astype(f32)
    for i, copy in enumerate(across[::-1]):
        copy.wait_recv()
        total = total + yrecv[i].astype(f32)
    projected = total.astype(bf16).astype(f32)
    stream = (skip[:, cols(lane)].astype(f32) + projected).astype(bf16)
    stream_out[...] = stream
    stream_f = stream.astype(f32)
    tok = stream_f.shape[0]
    square = jnp.sum(stream_f * stream_f, axis=1, keepdims=True)
    as_rows = jnp.broadcast_to(square, (tok, 128)).T[0:8, :]
    ssend[...] = as_rows
    sums = []
    for i in range(1, n_tp):
        sums.append(
            go(
                remote(
                    ssend, srecv.at[i - 1], ss.at[i - 1], sr.at[i - 1], (me, lax.rem(lane + i, n_tp))
                )
            )
        )
    for i, copy in enumerate(sums):
        copy.wait_recv()
        as_rows = as_rows + srecv[i]
    width = n_tp * d_local
    inv = lax.rsqrt(as_rows / width + EPS)
    inv_rms = jnp.broadcast_to(inv[0:1, :], (128, tok)).T[:, 0:1]
    normed = (stream_f * inv_rms * gain[0:1, cols(lane)]).astype(bf16)

    out_cols = cols(lane)
    arrivals = []
    for i in range(1, n_sp):
        to = lax.rem(me + i, n_sp)
        dsend[i - 1] = jnp.dot(hot[rows_of(to), :], normed, preferred_element_type=f32).astype(bf16)
        arrivals.append(
            go(
                remote(
                    dsend.at[i - 1], xs.at[rows_of(me), out_cols], ds.at[i - 1], dr.at[i - 1],
                    (to, lane),
                )
            )
        )
    xs[rows_of(me), out_cols] = jnp.dot(
        hot[rows_of(me), :], normed, preferred_element_type=f32
    ).astype(bf16)

    def spread(n, source):
        there = xs.at[rows_of(source), out_cols]
        for i in range(1, n_y):
            k = (i - 1) * n_sp + n
            go(remote(there, there, fs.at[k], fr.at[k], (me, y_at(i) * 2 + core)))
        go(remote(there, there, qs.at[n], qr.at[n], partner))

    def source_at(n):
        return lax.rem(me + n_sp - n, n_sp)

    def landed(source, block, recv, send):
        here = xs.at[rows_of(source), cols(block)]
        remote(here, here, send, recv, partner).wait_recv()

    spread(0, me)
    for n in range(1, n_sp):
        landed(source_at(n), lane, dr.at[n - 1], ds.at[n - 1])
        spread(n, source_at(n))
    for n in range(n_sp):
        for i in range(1, n_y):
            k = (i - 1) * n_sp + n
            from_block = lax.rem(y + n_y - i, n_y) * 2 + core
            landed(source_at(n), from_block, fr.at[k], fs.at[k])
            here = xs.at[rows_of(source_at(n)), cols(from_block)]
            q = i * n_sp + n
            go(remote(here, here, qs.at[q], qr.at[q], partner))
    for n in range(n_sp):
        for i in range(n_y):
            from_block = lax.rem(y + n_y - i, n_y) * 2 + 1 - core
            q = i * n_sp + n
            landed(source_at(n), from_block, qr.at[q], qs.at[q])
    for copy in waits:
        copy.wait_send()


def dispatch_call(rows, w, skip, gain, hot):
    n_sp, n_tp = lax.axis_size("sp"), lax.axis_size("tp")
    n_y = n_tp // 2
    bf16, f32 = jnp.bfloat16, jnp.float32
    tok, width = skip.shape
    d_local = width // n_tp
    slots = hot.shape[0]
    cap = slots // n_sp
    more = max(n_y - 1, 1)
    return pl.pallas_call(
        dispatch_kernel,
        out_shape=(
            jax.ShapeDtypeStruct((tok, d_local), bf16),
            jax.ShapeDtypeStruct((slots, width), bf16),
        ),
        in_specs=[VM] * 5,
        out_specs=(VM, VM),
        scratch_shapes=[
            pltpu.VMEM((n_y, tok, d_local), bf16),
            pltpu.VMEM((n_y, tok, d_local), bf16),
            pltpu.VMEM((more, tok, d_local), bf16),
            pltpu.VMEM((more, tok, d_local), bf16),
            pltpu.VMEM((8, tok), f32),
            pltpu.VMEM((n_tp - 1, 8, tok), f32),
            pltpu.VMEM((n_sp - 1, cap, d_local), bf16),
            DMA((n_y,)),
            DMA((n_y,)),
            DMA((more,)),
            DMA((more,)),
            DMA((n_tp - 1,)),
            DMA((n_tp - 1,)),
            DMA((n_sp - 1,)),
            DMA((n_sp - 1,)),
            DMA((more * n_sp,)),
            DMA((more * n_sp,)),
            DMA((n_y * n_sp,)),
            DMA((n_y * n_sp,)),
        ],
        compiler_params=pltpu.CompilerParams(
            collective_id=1, has_side_effects=True, vmem_limit_bytes=VMEM_ROOM // 2
        ),
        name="dispatch",
    )(rows, w, skip, gain, hot)


def return_kernel(
    hidden, w, share, pick,
    out,
    psend, own, precv, ysend, yrecv, rsend, ret,
    ps, pr, ys, yr, rs, rr,
):
    f32, bf16 = jnp.float32, jnp.bfloat16
    n_sp, n_tp, me, lane = places()
    n_y = n_tp // 2
    y, core = lane // 2, lax.rem(lane, 2)
    partner = (me, y * 2 + 1 - core)
    d_local = out.shape[1]
    cap = hidden.shape[0] // n_sp
    greet(
        [partner]
        + [(me, lax.rem(y + i, n_y) * 2 + core) for i in range(1, n_y)]
        + sp_peers(n_sp, me, lane)
    )

    def cols(block):
        return pl.ds(pl.multiple_of(block * d_local, 128), d_local)

    def rows_of(source):
        return pl.ds(pl.multiple_of(source * cap, 16), cap)

    def y_at(i):
        return lax.rem(y + i, n_y)

    def to_at(n):
        return lax.rem(me + n + 1, n_sp)

    waits = []

    def go(copy):
        copy.start()
        waits.append(copy)
        return copy

    pair, across, back = {}, {}, []
    def part(n, block):
        return jnp.dot(hidden[rows_of(to_at(n)), :], w[:, cols(block)], preferred_element_type=f32)

    order = list(range(1, n_y)) + [0]
    for n in range(n_sp + 1):
        if n < n_sp:
            for i in order:
                k = n * n_y + i
                psend[k] = part(n, y_at(i) * 2 + 1 - core).astype(bf16)
                pair[n, i] = go(remote(psend.at[k], precv.at[k], ps.at[k], pr.at[k], partner))
            for i in order:
                own[n * n_y + i] = part(n, y_at(i) * 2 + core)
        if n > 0:
            for i in range(1, n_y):
                pair[n - 1, i].wait_recv()
                j = (n - 1) * n_y + i
                k = (n - 1) * (n_y - 1) + i - 1
                ysend[k] = (own[j] + precv[j].astype(f32)).astype(bf16)
                across[n - 1, i] = go(
                    remote(
                        ysend.at[k], yrecv.at[k], ys.at[k], yr.at[k], (me, y_at(i) * 2 + core)
                    )
                )
    for n in range(n_sp):
        total = own[n * n_y]
        pair[n, 0].wait_recv()
        total = total + precv[n * n_y].astype(f32)
        for i in range(1, n_y):
            across[n, i].wait_recv()
            total = total + yrecv[n * (n_y - 1) + i - 1].astype(f32)
        if n < n_sp - 1:
            rsend[n] = total.astype(bf16)
            back.append(
                go(remote(rsend.at[n], ret.at[rows_of(me), :], rs.at[n], rr.at[n], (to_at(n), lane)))
            )
        else:
            ret[rows_of(me), :] = total.astype(bf16)
    for n in range(n_sp - 1):
        here = ret.at[rows_of(lax.rem(me + n_sp - n - 1, n_sp)), :]
        remote(here, here, rs.at[n], rr.at[n], partner).wait_recv()
    rows_in = ret[...]
    moe = None
    for k in range(pick.shape[0]):
        chosen = jnp.dot(pick[k], rows_in, preferred_element_type=f32) * share[:, k : k + 1]
        moe = chosen if moe is None else moe + chosen
    out[...] = moe
    for copy in waits:
        copy.wait_send()


def return_call(hidden, w, share, pick):
    n_sp, n_tp = lax.axis_size("sp"), lax.axis_size("tp")
    n_y = n_tp // 2
    bf16, f32 = jnp.bfloat16, jnp.float32
    tok, d_local = share.shape[0], w.shape[1] // n_tp
    slots = hidden.shape[0]
    cap = slots // n_sp
    more = max((n_y - 1) * n_sp, 1)
    return pl.pallas_call(
        return_kernel,
        out_shape=jax.ShapeDtypeStruct((tok, d_local), f32),
        in_specs=[VM] * 4,
        out_specs=VM,
        scratch_shapes=[
            pltpu.VMEM((n_y * n_sp, cap, d_local), bf16),
            pltpu.VMEM((n_y * n_sp, cap, d_local), f32),
            pltpu.VMEM((n_y * n_sp, cap, d_local), bf16),
            pltpu.VMEM((more, cap, d_local), bf16),
            pltpu.VMEM((more, cap, d_local), bf16),
            pltpu.VMEM((n_sp - 1, cap, d_local), bf16),
            pltpu.VMEM((slots, d_local), bf16),
            DMA((n_y * n_sp,)),
            DMA((n_y * n_sp,)),
            DMA((more,)),
            DMA((more,)),
            DMA((n_sp - 1,)),
            DMA((n_sp - 1,)),
        ],
        compiler_params=pltpu.CompilerParams(
            collective_id=2, has_side_effects=True, vmem_limit_bytes=VMEM_ROOM
        ),
        name="combine",
    )(hidden, w, share, pick)


def per_device(
    lane_source_signal,
    spectral_damping_part,
    spectral_angular_part,
    interval_exponent,
    entry_matrix_inphase,
    entry_matrix_quadrature,
    emission_inphase,
    emission_quadrature,
    lane_bypass_factor,
    spike_shrink_offset,
    lane_exit_matrix,
    skipline_stream,
    specialist_scaling_vector,
    selected_specialists,
    dispatcher_scores,
    specialist_valve_matrix,
    specialist_widen_matrix,
    specialist_shrink_matrix,
):
    f32, bf16 = jnp.float32, jnp.bfloat16
    gs = entry_matrix_inphase.shape[2]
    p_size = spectral_damping_part.shape[1]
    mixed, hot, pick, share = mixer_call(
        lane_source_signal,
        spectral_damping_part,
        spectral_angular_part,
        interval_exponent[None, :],
        entry_matrix_inphase.reshape(-1, gs),
        entry_matrix_quadrature.reshape(-1, gs),
        emission_inphase.reshape(-1, p_size),
        emission_quadrature.reshape(-1, p_size),
        lane_bypass_factor[None, :],
        spike_shrink_offset,
        selected_specialists,
        dispatcher_scores,
    )
    stream, rows = dispatch_call(
        mixed,
        lane_exit_matrix,
        skipline_stream,
        specialist_scaling_vector[None, :],
        hot,
    )
    gate_part = jnp.dot(rows, specialist_valve_matrix[0], preferred_element_type=f32)
    up_part = jnp.dot(rows, specialist_widen_matrix[0], preferred_element_type=f32)
    hidden = (jax.nn.silu(gate_part) * up_part).astype(bf16)
    moe = return_call(hidden, specialist_shrink_matrix[0], share, pick)
    return (stream.astype(f32) + moe).astype(bf16)


def solution(mesh):
    placed = (
        P("tp", "sp"),
        P("tp", None),
        P("tp", None),
        P("tp"),
        P("tp", None, None),
        P("tp", None, None),
        P("tp", None, None),
        P("tp", None, None),
        P("tp"),
        P("tp", "sp"),
        P("tp", None),
        P("sp", None),
        P(),
        P("sp", None),
        P("sp", None),
        P("sp", None, "tp"),
        P("sp", None, "tp"),
        P("sp", "tp", None),
    )
    return jax.shard_map(
        per_device, mesh=mesh, in_specs=placed, out_specs=P("sp", "tp"), check_vma=False
    )
```

```python
import jax
import jax.numpy as jnp
from jax import lax
from jax.experimental import pallas as pl
from jax.experimental.pallas import tpu as pltpu
from jax.sharding import PartitionSpec as P

EPS = 1e-06
MESH = pl.DeviceIdType.MESH
VM = pl.BlockSpec(memory_space=pltpu.VMEM)
FAR = pl.BlockSpec(memory_space=pl.ANY)
DMA = pltpu.SemaphoreType.DMA
VMEM_ROOM = 60 * 1024 * 1024
HIGH, HIGHEST = lax.Precision.HIGH, lax.Precision.HIGHEST
GROUP = 128


def remote(src, dst, send, recv, where):
    return pltpu.make_async_remote_copy(
        src_ref=src, dst_ref=dst, send_sem=send, recv_sem=recv, device_id=where, device_id_type=MESH
    )


def places():
    n_sp, n_tp = lax.axis_size("sp"), lax.axis_size("tp")
    return n_sp, n_tp, lax.axis_index("sp"), lax.axis_index("tp")


def xor(a, b, n):
    out, bit = 0, 1
    while bit < n:
        p, q = lax.rem(lax.div(a, bit), 2), (b // bit) % 2
        out = out + bit * (p + q - 2 * p * q)
        bit *= 2
    return out


def dot(a, b, precision=None):
    return jnp.dot(a, b, precision=precision, preferred_element_type=jnp.float32)


def dot_nt(a, b, precision=None):
    return lax.dot_general(
        a, b, (((1,), (1,)), ((), ())), precision=precision, preferred_element_type=jnp.float32
    )


def iota(shape, dim):
    return lax.broadcasted_iota(jnp.int32, shape, dim)


def where_one(mask):
    return jnp.where(mask, 1.0, 0.0)


def expm1_of(x):
    series = jnp.ones_like(x)
    for k in range(11, 1, -1):
        series = 1.0 + x * series * (1.0 / k)
    return jnp.where(jnp.abs(x) < 0.7, x * series, jnp.exp(x) - 1.0)


def affine_pair(earlier, latter):
    mul_re = earlier[0] * latter[0] - earlier[1] * latter[1]
    mul_im = earlier[0] * latter[1] + earlier[1] * latter[0]
    add_re = latter[0] * earlier[2] - latter[1] * earlier[3] + latter[2]
    add_im = latter[0] * earlier[3] + latter[1] * earlier[2] + latter[3]
    return (mul_re, mul_im, add_re, add_im)


N_IN = 18


def layer_kernel(*refs):
    f32, bf16 = jnp.float32, jnp.bfloat16
    far = refs[:N_IN]
    out = refs[N_IN]
    near = refs[N_IN + 1 : 2 * N_IN + 1]
    (
        fetched, xr, xi, cr, ci, mine, pieces, mixed_s, hot, weigh, stream_s,
        psend_a, precv_a, ysend_a, yrecv_a, ssend, srecv,
        xs, dsend, psend, own, precv, ysend, yrecv, rsend, ret,
        carry_s, carry_r, pa_s, pa_r, ya_s, ya_r, sum_s, sum_r, d_s, d_r,
        f_s, f_r, q_s, q_r, p_s, p_r, y_s, y_r, r_s, r_r,
    ) = refs[2 * N_IN + 1 :]
    (
        u, damp, ang, log_dt, ent_re, ent_im, emi_re, emi_im, bypass, shrink, sel, scores,
        w, skip, gain, wg, wu, wd,
    ) = near
    n_sp, n_tp, me, lane = places()
    n_y = n_tp // 2
    y, core = lax.div(lane, 2), lax.rem(lane, 2)
    partner = (me, y * 2 + 1 - core)
    tok, d_local = out.shape
    slots, width = xs.shape
    cap = slots // n_sp
    per_group = GROUP // cap
    n_groups = slots // GROUP

    def cols(block):
        return pl.ds(pl.multiple_of(block * d_local, 128), d_local)

    def peer(k):
        return (xor(me, k, n_sp), lane)

    def rows_of(k):
        return slice(k * cap, k * cap + cap)

    def y_at(i):
        return lax.rem(y + i, n_y)

    def across_y(i):
        return (me, y_at(i) * 2 + core)

    barrier = pltpu.get_barrier_semaphore()
    peers = [(me, lax.rem(lane + i, n_tp)) for i in range(1, n_tp)]
    peers += [(lax.rem(me + i, n_sp), lane) for i in range(1, n_sp)]
    for other in peers:
        pl.semaphore_signal(barrier, inc=1, device_id=other, device_id_type=MESH)

    def fetch(i):
        src = far[i]
        if i == 13:
            src = src.at[:, cols(lane)]
        return pltpu.make_async_copy(src, near[i], fetched.at[i])

    for i in range(N_IN):
        fetch(i).start()
    for i in range(12):
        fetch(i).wait()

    waits = []

    def go(copy):
        copy.start()
        waits.append(copy)
        return copy

    groups, p_size = damp.shape
    chans = u.shape[0]
    gs = chans // groups
    states = groups * p_size
    tiles = states // 128
    per = 128 // p_size
    n_j = 8
    n_i = tok // n_j

    def lane_group(rows):
        return iota((rows, 128), 1) // p_size

    def as_row(a):
        wide = jnp.concatenate([a] * per, axis=1)
        parts = []
        for tile in range(tiles):
            row = wide[per * tile : per * tile + 1]
            for k in range(1, per):
                row = jnp.where(lane_group(1) == k, wide[per * tile + k : per * tile + k + 1], row)
            parts.append(row)
        return jnp.concatenate(parts, axis=1)

    def spread_tile(columns, tile):
        value = jnp.broadcast_to(columns[:, per * tile : per * tile + 1], (tok, 128))
        for k in range(1, per):
            other = jnp.broadcast_to(columns[:, per * tile + k : per * tile + k + 1], (tok, 128))
            value = jnp.where(lane_group(tok) == k, other, value)
        return value

    block_mask = iota((chans, states), 1) // p_size == iota((chans, states), 0) // gs

    def block_diagonal(a):
        wide = jnp.concatenate([a] * per, axis=1)
        return jnp.where(block_mask, jnp.concatenate([wide] * tiles, axis=1), 0.0)

    eye = where_one(iota((groups, groups), 0) == iota((groups, groups), 1))
    dt = jnp.exp(jnp.sum(eye * log_dt[...], axis=1, keepdims=True))
    a_re, a_im = damp[...], ang[...]
    log_rate = a_re * dt
    angle = a_im * dt
    cos, sin = jnp.cos(angle), jnp.sin(angle)
    half = jnp.sin(0.5 * angle)
    decay = jnp.exp(log_rate)
    num_re = expm1_of(log_rate) * cos - 2.0 * half * half
    num_im = decay * sin
    denom = a_re * a_re + a_im * a_im
    fac_re = as_row((num_re * a_re + num_im * a_im) / denom)
    fac_im = as_row((num_im * a_re - num_re * a_im) / denom)
    lam_re = as_row(decay * cos)
    lam_im = as_row(decay * sin)

    order = iota((tok, tok), 0)
    perm = where_one((order % n_j) * n_i + order // n_j == iota((tok, tok), 1))
    columns = jnp.exp(dot_nt(perm, shrink[...], HIGHEST))
    signal = dot_nt(perm.astype(bf16), u[...])
    in_re, in_im = block_diagonal(ent_re[...]), block_diagonal(ent_im[...])
    drive_re = dot(signal, fac_re * in_re - fac_im * in_im, HIGH)
    drive_im = dot(signal, fac_re * in_im + fac_im * in_re, HIGH)
    row_j = iota((n_j, 128), 0)
    ends = []
    for tile in range(tiles):
        at = slice(128 * tile, 128 * tile + 128)
        modulus = spread_tile(columns, tile)
        t_re, t_im = modulus * lam_re[:, at], modulus * lam_im[:, at]
        for i in range(n_i):
            step = slice(n_j * i, n_j * i + n_j)
            now = (t_re[step], t_im[step], drive_re[step, at], drive_im[step, at])
            run = now if i == 0 else affine_pair(run, now)
            for ref, value in zip((cr, ci, xr, xi), run):
                ref[step, at] = value
        off = 1
        while off < n_j:
            before = [pltpu.roll(value, off, 0) for value in run]
            joined = affine_pair(before, run)
            run = tuple(jnp.where(row_j >= off, new, old) for new, old in zip(joined, run))
            off *= 2
        for plane in range(4):
            mine[plane, tile : tile + 1, :] = run[plane][n_j - 1 : n_j]
        fills = (1.0, 0.0, 0.0, 0.0)
        ends.append(
            [jnp.where(row_j >= 1, pltpu.roll(v, 1, 0), fill) for v, fill in zip(run, fills)]
        )

    pl.semaphore_wait(barrier, len(peers))

    def carry_copy(i):
        return remote(
            mine, pieces.at[i - 1], carry_s.at[i - 1], carry_r.at[i - 1],
            (lax.rem(me + i, n_sp), lane),
        )

    for i in range(1, n_sp):
        @pl.when(me + i < n_sp)
        def _(i=i):
            carry_copy(i).start()

    top = sel.shape[0]
    eye_t = where_one(iota((tok, tok), 0) == iota((tok, tok), 1))
    chosen = dot_nt(eye_t.astype(bf16), sel[...].astype(f32).astype(bf16))
    share = dot_nt(eye_t, scores[...] / jnp.sum(scores[...], axis=0, keepdims=True), HIGHEST)
    index = iota((1, GROUP), 1)
    expert = jnp.where(index < n_sp, xor(me, index, n_sp), -1).astype(f32)
    choice = [chosen[:, k : k + 1] == expert for k in range(top)]
    member = where_one(choice[0])
    part_of = jnp.where(choice[0], share[:, 0:1], 0.0)
    for k in range(1, top):
        member = jnp.where(choice[k], 1.0, member)
        part_of = jnp.where(choice[k], share[:, k : k + 1], part_of)
    below = where_one(iota((tok, tok), 1) <= iota((tok, tok), 0)).astype(bf16)
    rank = (dot(below, member.astype(bf16)) * member).astype(bf16)
    of_slot = where_one(iota((slots, GROUP), 0) // cap == iota((slots, GROUP), 1)).astype(bf16)
    want = (iota((slots, tok), 0) % cap + 1).astype(f32)
    hot[...] = where_one(dot_nt(of_slot, rank) == want).astype(bf16)
    want = (iota((tok, slots), 1) % cap + 1).astype(f32)
    at_slot = dot_nt(part_of.astype(bf16), of_slot)
    weigh[...] = jnp.where(dot_nt(rank, of_slot) == want, at_slot, 0.0).astype(bf16)

    q_re, q_im = block_diagonal(emi_re[...]), block_diagonal(emi_im[...])

    for i in range(1, n_sp):
        @pl.when(me >= i)
        def _(i=i):
            carry_copy(i).wait_recv()
    run_re = jnp.zeros(mine.shape[1:], f32)
    run_im = run_re
    for i in range(n_sp - 1, 0, -1):
        mul_re, mul_im, add_re, add_im = (pieces[i - 1, plane] for plane in range(4))
        new_re = mul_re * run_re - mul_im * run_im + add_re
        new_im = mul_re * run_im + mul_im * run_re + add_im
        run_re = jnp.where(me >= i, new_re, run_re)
        run_im = jnp.where(me >= i, new_im, run_im)

    for tile in range(tiles):
        at = slice(128 * tile, 128 * tile + 128)
        p_re, p_im, z_re, z_im = ends[tile]
        e_re, e_im = run_re[tile : tile + 1], run_im[tile : tile + 1]
        z_re = z_re + p_re * e_re - p_im * e_im
        z_im = z_im + p_re * e_im + p_im * e_re
        for i in range(n_i):
            step = slice(n_j * i, n_j * i + n_j)
            c_re, c_im = cr[step, at], ci[step, at]
            xr[step, at] = xr[step, at] + c_re * z_re - c_im * z_im
            xi[step, at] = xi[step, at] + c_re * z_im + c_im * z_re
    value = dot_nt(xr[...], q_re, HIGH) - dot_nt(xi[...], q_im, HIGH) + signal * bypass[...]
    order = iota((tok, tok), 1)
    back = where_one((order % n_j) * n_i + order // n_j == iota((tok, tok), 0)).astype(bf16)
    mixed_s[...] = dot(back, jax.nn.gelu(value).astype(bf16)).astype(bf16)

    for i in range(12, 15):
        fetch(i).wait()

    def projected_part(block):
        return dot(mixed_s[...], w[:, cols(block)])

    pair = {}
    for i in range(n_y - 1, -1, -1):
        psend_a[i] = projected_part(y_at(i) * 2 + 1 - core).astype(bf16)
        pair[i] = go(remote(psend_a.at[i], precv_a.at[i], pa_s.at[i], pa_r.at[i], partner))
    across = {}
    for i in range(n_y - 1, 0, -1):
        part = projected_part(y_at(i) * 2 + core)
        pair[i].wait_recv()
        ysend_a[i - 1] = (part + precv_a[i].astype(f32)).astype(bf16)
        across[i] = go(
            remote(
                ysend_a.at[i - 1], yrecv_a.at[i - 1], ya_s.at[i - 1], ya_r.at[i - 1], across_y(i)
            )
        )
    total = projected_part(lane)
    pair[0].wait_recv()
    total = total + precv_a[0].astype(f32)
    for i in range(1, n_y):
        across[i].wait_recv()
        total = total + yrecv_a[i - 1].astype(f32)
    stream = (skip[...].astype(f32) + total.astype(bf16).astype(f32)).astype(bf16)
    stream_s[...] = stream
    stream_f = stream.astype(f32)
    square = jnp.sum(stream_f * stream_f, axis=1, keepdims=True)
    as_rows = jnp.broadcast_to(square, (tok, 128)).T[0:8, :]
    ssend[...] = as_rows
    sums = []
    for i in range(1, n_tp):
        sums.append(
            go(
                remote(
                    ssend, srecv.at[i - 1], sum_s.at[i - 1], sum_r.at[i - 1],
                    (me, lax.rem(lane + i, n_tp)),
                )
            )
        )
    scaled = stream_f * gain[0:1, cols(lane)]
    for i, copy in enumerate(sums):
        copy.wait_recv()
        as_rows = as_rows + srecv[i]
    inv = lax.rsqrt(as_rows / width + EPS)
    inv_rms = jnp.broadcast_to(inv[0:1, :], (128, tok)).T[:, 0:1]
    normed = (scaled * inv_rms).astype(bf16)

    def put(k):
        return dot(hot[rows_of(k), :], normed).astype(bf16)

    mine_cols = cols(lane)

    def forward(k):
        here = xs.at[rows_of(k), mine_cols]
        for i in range(1, n_y):
            n = k * (n_y - 1) + i - 1
            go(remote(here, here, f_s.at[n], f_r.at[n], across_y(i)))
        go(remote(here, here, q_s.at[k * n_y], q_r.at[k * n_y], partner))

    xs[rows_of(0), mine_cols] = put(0)
    forward(0)
    for k in range(1, n_sp):
        dsend[k - 1] = put(k)
        go(
            remote(
                dsend.at[k - 1], xs.at[rows_of(k), mine_cols], d_s.at[k - 1], d_r.at[k - 1], peer(k)
            )
        )

    def landed(k, block, send, recv):
        here = xs.at[rows_of(k), cols(block)]
        remote(here, here, send, recv, partner).wait_recv()

    def members(m):
        return range(m * per_group, m * per_group + per_group)

    def step_a(m):
        for k in members(m):
            if k > 0:
                landed(k, lane, d_s.at[k - 1], d_r.at[k - 1])
                forward(k)

    def from_y(i):
        return lax.rem(y + n_y - i, n_y)

    def step_b(m):
        for k in members(m):
            for i in range(1, n_y):
                n = k * (n_y - 1) + i - 1
                block = from_y(i) * 2 + core
                landed(k, block, f_s.at[n], f_r.at[n])
                here = xs.at[rows_of(k), cols(block)]
                go(remote(here, here, q_s.at[k * n_y + i], q_r.at[k * n_y + i], partner))

    pairs, acrosses, backs = {}, {}, {}

    def step_c(m):
        for k in members(m):
            for i in range(n_y):
                block = from_y(i) * 2 + 1 - core
                landed(k, block, q_s.at[k * n_y + i], q_r.at[k * n_y + i])
        rows = xs[m * GROUP : m * GROUP + GROUP, :]
        gate = dot(rows, wg[...])
        hidden = (jax.nn.silu(gate) * dot(rows, wu[...])).astype(bf16)
        order = list(range(1, n_y)) + [0]
        for i in order:
            n = m * n_y + i
            psend[n] = dot(hidden, wd[:, cols(y_at(i) * 2 + 1 - core)]).astype(bf16)
            pairs[n] = go(remote(psend.at[n], precv.at[n], p_s.at[n], p_r.at[n], partner))
        for i in order:
            own[m * n_y + i] = dot(hidden, wd[:, cols(y_at(i) * 2 + core)])

    def step_d(m):
        for i in range(1, n_y):
            n, j = m * n_y + i, m * (n_y - 1) + i - 1
            pairs[n].wait_recv()
            ysend[j] = (own[n] + precv[n].astype(f32)).astype(bf16)
            for k in reversed(members(m)):
                at = pl.ds((k % per_group) * cap, cap)
                s = k * (n_y - 1) + i - 1
                acrosses[k, i] = go(
                    remote(ysend.at[j, at], yrecv.at[j, at], y_s.at[s], y_r.at[s], across_y(i))
                )

    def step_e(m):
        pairs[m * n_y].wait_recv()
        for k in reversed(members(m)):
            at = slice((k % per_group) * cap, (k % per_group) * cap + cap)
            total = own[m * n_y, at] + precv[m * n_y, at].astype(f32)
            for i in range(1, n_y):
                acrosses[k, i].wait_recv()
                total = total + yrecv[m * (n_y - 1) + i - 1, at].astype(f32)
            if k > 0:
                rsend[k - 1] = total.astype(bf16)
                backs[k] = go(
                    remote(
                        rsend.at[k - 1], ret.at[rows_of(k)], r_s.at[k - 1], r_r.at[k - 1], peer(k)
                    )
                )
            else:
                ret[rows_of(0), :] = total.astype(bf16)

    step_a(0)
    step_a(1)
    step_b(0)
    step_b(1)
    step_a(2)
    for i in range(15, 18):
        fetch(i).wait()
    step_c(1)
    step_b(2)
    step_d(1)
    step_a(3)
    step_c(2)
    step_d(2)
    step_b(3)
    step_e(1)
    step_c(3)
    step_d(3)
    step_c(0)
    step_d(0)
    step_e(2)
    step_e(3)
    step_e(0)
    total = stream_s[...].astype(f32)
    for m in list(range(1, n_groups)) + [0]:
        for k in members(m):
            if k > 0:
                backs[k].wait_recv()
        at = slice(m * GROUP, m * GROUP + GROUP)
        total = total + dot(weigh[:, at], ret[at, :])
    out[...] = total.astype(bf16)
    for copy in waits:
        copy.wait_send()
    for i in range(1, n_sp):
        @pl.when(me + i < n_sp)
        def _(i=i):
            carry_copy(i).wait_send()


def layer_call(*args):
    n_sp, n_tp = lax.axis_size("sp"), lax.axis_size("tp")
    n_y = n_tp // 2
    f32, bf16 = jnp.float32, jnp.bfloat16
    tok, width = args[13].shape
    d_local = width // n_tp
    chans = args[0].shape[0]
    groups, p_size = args[1].shape
    states = groups * p_size
    slots = 2 * tok * args[10].shape[0]
    cap = slots // n_sp
    n_groups = slots // GROUP
    more = max(n_y - 1, 1)
    plane = (4, states // 128, 128)
    room = [pltpu.VMEM(a.shape, a.dtype) for a in args]
    room[13] = pltpu.VMEM((tok, d_local), bf16)
    pairs = [n_sp - 1, n_y, more, n_tp - 1, n_sp - 1, n_sp * more, n_sp * n_y, n_groups * n_y]
    pairs += [n_sp * more, n_sp - 1]
    return pl.pallas_call(
        layer_kernel,
        out_shape=jax.ShapeDtypeStruct((tok, d_local), bf16),
        in_specs=[FAR] * N_IN,
        out_specs=VM,
        scratch_shapes=room
        + [DMA((N_IN,))]
        + [pltpu.VMEM((tok, states), f32)] * 4
        + [
            pltpu.VMEM(plane, f32),
            pltpu.VMEM((n_sp - 1,) + plane, f32),
            pltpu.VMEM((tok, chans), bf16),
            pltpu.VMEM((slots, tok), bf16),
            pltpu.VMEM((tok, slots), bf16),
            pltpu.VMEM((tok, d_local), bf16),
            pltpu.VMEM((n_y, tok, d_local), bf16),
            pltpu.VMEM((n_y, tok, d_local), bf16),
            pltpu.VMEM((more, tok, d_local), bf16),
            pltpu.VMEM((more, tok, d_local), bf16),
            pltpu.VMEM((8, tok), f32),
            pltpu.VMEM((n_tp - 1, 8, tok), f32),
            pltpu.VMEM((slots, width), bf16),
            pltpu.VMEM((n_sp - 1, cap, d_local), bf16),
            pltpu.VMEM((n_groups * n_y, GROUP, d_local), bf16),
            pltpu.VMEM((n_groups * n_y, GROUP, d_local), f32),
            pltpu.VMEM((n_groups * n_y, GROUP, d_local), bf16),
            pltpu.VMEM((n_groups * more, GROUP, d_local), bf16),
            pltpu.VMEM((n_groups * more, GROUP, d_local), bf16),
            pltpu.VMEM((n_sp - 1, cap, d_local), bf16),
            pltpu.VMEM((slots, d_local), bf16),
        ]
        + [DMA((n,)) for n in pairs for _ in range(2)],
        compiler_params=pltpu.CompilerParams(
            collective_id=0, has_side_effects=True, vmem_limit_bytes=VMEM_ROOM
        ),
        name="layer",
    )(*args)


def per_device(
    lane_source_signal,
    spectral_damping_part,
    spectral_angular_part,
    interval_exponent,
    entry_matrix_inphase,
    entry_matrix_quadrature,
    emission_inphase,
    emission_quadrature,
    lane_bypass_factor,
    spike_shrink_offset,
    lane_exit_matrix,
    skipline_stream,
    specialist_scaling_vector,
    selected_specialists,
    dispatcher_scores,
    specialist_valve_matrix,
    specialist_widen_matrix,
    specialist_shrink_matrix,
):
    p_size = spectral_damping_part.shape[1]
    return layer_call(
        lane_source_signal,
        spectral_damping_part,
        spectral_angular_part,
        interval_exponent[None, :],
        jnp.swapaxes(entry_matrix_inphase, 1, 2).reshape(-1, p_size),
        jnp.swapaxes(entry_matrix_quadrature, 1, 2).reshape(-1, p_size),
        emission_inphase.reshape(-1, p_size),
        emission_quadrature.reshape(-1, p_size),
        lane_bypass_factor[None, :],
        spike_shrink_offset,
        selected_specialists.T,
        dispatcher_scores.T,
        lane_exit_matrix,
        skipline_stream,
        specialist_scaling_vector[None, :],
        specialist_valve_matrix[0],
        specialist_widen_matrix[0],
        specialist_shrink_matrix[0],
    )


def solution(mesh):
    placed = (
        P("tp", "sp"),
        P("tp", None),
        P("tp", None),
        P("tp"),
        P("tp", None, None),
        P("tp", None, None),
        P("tp", None, None),
        P("tp", None, None),
        P("tp"),
        P("tp", "sp"),
        P("tp", None),
        P("sp", None),
        P(),
        P("sp", None),
        P("sp", None),
        P("sp", None, "tp"),
        P("sp", None, "tp"),
        P("sp", "tp", None),
    )
    return jax.shard_map(
        per_device, mesh=mesh, in_specs=placed, out_specs=P("sp", "tp"), check_vma=False
    )
```

```python
import jax
import jax.numpy as jnp
from jax import lax
from jax.experimental import pallas as pl
from jax.experimental.pallas import tpu as pltpu
from jax.sharding import PartitionSpec as P

EPS = 1e-06
MESH = pl.DeviceIdType.MESH
VM = pl.BlockSpec(memory_space=pltpu.VMEM)
FAR = pl.BlockSpec(memory_space=pl.ANY)
DMA = pltpu.SemaphoreType.DMA
VMEM_ROOM = 60 * 1024 * 1024
HIGH, HIGHEST = lax.Precision.HIGH, lax.Precision.HIGHEST
GROUP = 128


def remote(src, dst, send, recv, where):
    return pltpu.make_async_remote_copy(
        src_ref=src, dst_ref=dst, send_sem=send, recv_sem=recv, device_id=where, device_id_type=MESH
    )


def places():
    n_sp, n_tp = lax.axis_size("sp"), lax.axis_size("tp")
    return n_sp, n_tp, lax.axis_index("sp"), lax.axis_index("tp")


def xor(a, b, n):
    out, bit = 0, 1
    while bit < n:
        p, q = lax.rem(lax.div(a, bit), 2), (b // bit) % 2
        out = out + bit * (p + q - 2 * p * q)
        bit *= 2
    return out


def dot(a, b, precision=None):
    return jnp.dot(a, b, precision=precision, preferred_element_type=jnp.float32)


def dot_nt(a, b, precision=None):
    return lax.dot_general(
        a, b, (((1,), (1,)), ((), ())), precision=precision, preferred_element_type=jnp.float32
    )


def iota(shape, dim):
    return lax.broadcasted_iota(jnp.int32, shape, dim)


def where_one(mask):
    return jnp.where(mask, 1.0, 0.0)


def expm1_of(x):
    series = jnp.ones_like(x)
    for k in range(11, 1, -1):
        series = 1.0 + x * series * (1.0 / k)
    return jnp.where(jnp.abs(x) < 0.7, x * series, jnp.exp(x) - 1.0)


def affine_pair(earlier, latter):
    mul_re = earlier[0] * latter[0] - earlier[1] * latter[1]
    mul_im = earlier[0] * latter[1] + earlier[1] * latter[0]
    add_re = latter[0] * earlier[2] - latter[1] * earlier[3] + latter[2]
    add_im = latter[0] * earlier[3] + latter[1] * earlier[2] + latter[3]
    return (mul_re, mul_im, add_re, add_im)


N_IN = 18


def layer_kernel(*refs):
    f32, bf16 = jnp.float32, jnp.bfloat16
    far = refs[:N_IN]
    out = refs[N_IN]
    near = refs[N_IN + 1 : 2 * N_IN + 1]
    (
        fetched, xr, xi, cr, ci, mine, pieces, mixed_s, hot, weigh, stream_s,
        psend_a, precv_a, ysend_a, yrecv_a, ssend, srecv,
        xs, nsend, nrecv, dsend, psend, own, precv, ysend, yrecv, rsend, ret,
        carry_s, carry_r, n_s, n_r, pa_s, pa_r, ya_s, ya_r, sum_s, sum_r, d_s, d_r,
        f_s, f_r, q_s, q_r, p_s, p_r, y_s, y_r, r_s, r_r,
    ) = refs[2 * N_IN + 1 :]
    (
        u, damp, ang, log_dt, ent_re, ent_im, emi_re, emi_im, bypass, shrink, sel, scores,
        w, skip, gain, wg, wu, wd,
    ) = near
    n_sp, n_tp, me, lane = places()
    n_y = n_tp // 2
    y, core = lax.div(lane, 2), lax.rem(lane, 2)
    partner = (me, y * 2 + 1 - core)
    tok, d_local = out.shape
    slots, width = xs.shape
    cap = slots // n_sp
    per_group = GROUP // cap
    n_groups = slots // GROUP

    def cols(block):
        return pl.ds(pl.multiple_of(block * d_local, 128), d_local)

    def peer(k):
        return (xor(me, k, n_sp), lane)

    def rows_of(k):
        return slice(k * cap, k * cap + cap)

    def y_at(i):
        return lax.rem(y + i, n_y)

    def across_y(i):
        return (me, y_at(i) * 2 + core)

    barrier = pltpu.get_barrier_semaphore()
    peers = [(me, lax.rem(lane + i, n_tp)) for i in range(1, n_tp)]
    peers += [(lax.rem(me + i, n_sp), lane) for i in range(1, n_sp)]
    for other in peers:
        pl.semaphore_signal(barrier, inc=1, device_id=other, device_id_type=MESH)

    def fetch(i):
        src = far[i]
        if i == 13:
            src = src.at[:, cols(lane)]
        return pltpu.make_async_copy(src, near[i], fetched.at[i])

    for i in range(N_IN):
        fetch(i).start()
    for i in range(12):
        fetch(i).wait()

    waits = []

    def go(copy):
        copy.start()
        waits.append(copy)
        return copy

    groups, p_size = damp.shape
    chans = u.shape[0]
    gs = chans // groups
    states = groups * p_size
    tiles = states // 128
    per = 128 // p_size
    n_j = 8
    n_i = tok // n_j

    def lane_group(rows):
        return iota((rows, 128), 1) // p_size

    def as_row(a):
        wide = jnp.concatenate([a] * per, axis=1)
        parts = []
        for tile in range(tiles):
            row = wide[per * tile : per * tile + 1]
            for k in range(1, per):
                row = jnp.where(lane_group(1) == k, wide[per * tile + k : per * tile + k + 1], row)
            parts.append(row)
        return jnp.concatenate(parts, axis=1)

    def spread_tile(columns, tile):
        value = jnp.broadcast_to(columns[:, per * tile : per * tile + 1], (tok, 128))
        for k in range(1, per):
            other = jnp.broadcast_to(columns[:, per * tile + k : per * tile + k + 1], (tok, 128))
            value = jnp.where(lane_group(tok) == k, other, value)
        return value

    block_mask = iota((chans, states), 1) // p_size == iota((chans, states), 0) // gs

    def block_diagonal(a):
        wide = jnp.concatenate([a] * per, axis=1)
        return jnp.where(block_mask, jnp.concatenate([wide] * tiles, axis=1), 0.0)

    eye = where_one(iota((groups, groups), 0) == iota((groups, groups), 1))
    dt = jnp.exp(jnp.sum(eye * log_dt[...], axis=1, keepdims=True))
    a_re, a_im = damp[...], ang[...]
    log_rate = a_re * dt
    angle = a_im * dt
    cos, sin = jnp.cos(angle), jnp.sin(angle)
    half = jnp.sin(0.5 * angle)
    decay = jnp.exp(log_rate)
    num_re = expm1_of(log_rate) * cos - 2.0 * half * half
    num_im = decay * sin
    denom = a_re * a_re + a_im * a_im
    fac_re = as_row((num_re * a_re + num_im * a_im) / denom)
    fac_im = as_row((num_im * a_re - num_re * a_im) / denom)
    lam_re = as_row(decay * cos)
    lam_im = as_row(decay * sin)

    order = iota((tok, tok), 0)
    perm = where_one((order % n_j) * n_i + order // n_j == iota((tok, tok), 1))
    columns = jnp.exp(dot_nt(perm, shrink[...], HIGHEST))
    signal = dot_nt(perm.astype(bf16), u[...])
    in_re, in_im = block_diagonal(ent_re[...]), block_diagonal(ent_im[...])
    drive_re = dot(signal, fac_re * in_re - fac_im * in_im, HIGH)
    drive_im = dot(signal, fac_re * in_im + fac_im * in_re, HIGH)
    row_j = iota((n_j, 128), 0)
    ends = []
    for tile in range(tiles):
        at = slice(128 * tile, 128 * tile + 128)
        modulus = spread_tile(columns, tile)
        t_re, t_im = modulus * lam_re[:, at], modulus * lam_im[:, at]
        for i in range(n_i):
            step = slice(n_j * i, n_j * i + n_j)
            now = (t_re[step], t_im[step], drive_re[step, at], drive_im[step, at])
            run = now if i == 0 else affine_pair(run, now)
            for ref, value in zip((cr, ci, xr, xi), run):
                ref[step, at] = value
        off = 1
        while off < n_j:
            before = [pltpu.roll(value, off, 0) for value in run]
            joined = affine_pair(before, run)
            run = tuple(jnp.where(row_j >= off, new, old) for new, old in zip(joined, run))
            off *= 2
        for plane in range(4):
            mine[plane, tile : tile + 1, :] = run[plane][n_j - 1 : n_j]
        fills = (1.0, 0.0, 0.0, 0.0)
        ends.append(
            [jnp.where(row_j >= 1, pltpu.roll(v, 1, 0), fill) for v, fill in zip(run, fills)]
        )

    pl.semaphore_wait(barrier, len(peers))

    def carry_copy(i):
        return remote(
            mine, pieces.at[i - 1], carry_s.at[i - 1], carry_r.at[i - 1],
            (lax.rem(me + i, n_sp), lane),
        )

    for i in range(1, n_sp):
        @pl.when(me + i < n_sp)
        def _(i=i):
            carry_copy(i).start()

    top = sel.shape[0]
    eye_t = where_one(iota((tok, tok), 0) == iota((tok, tok), 1))
    chosen = dot_nt(eye_t.astype(bf16), sel[...].astype(f32).astype(bf16))
    share = dot_nt(eye_t, scores[...] / jnp.sum(scores[...], axis=0, keepdims=True), HIGHEST)
    index = iota((1, GROUP), 1)
    expert = jnp.where(index < n_sp, xor(me, index, n_sp), -1).astype(f32)
    choice = [chosen[:, k : k + 1] == expert for k in range(top)]
    member = where_one(choice[0])
    part_of = jnp.where(choice[0], share[:, 0:1], 0.0)
    for k in range(1, top):
        member = jnp.where(choice[k], 1.0, member)
        part_of = jnp.where(choice[k], share[:, k : k + 1], part_of)
    below = where_one(iota((tok, tok), 1) <= iota((tok, tok), 0)).astype(bf16)
    rank = (dot(below, member.astype(bf16)) * member).astype(bf16)
    of_slot = where_one(iota((slots, GROUP), 0) // cap == iota((slots, GROUP), 1)).astype(bf16)
    want = (iota((slots, tok), 0) % cap + 1).astype(f32)
    hot[...] = where_one(dot_nt(of_slot, rank) == want).astype(bf16)
    want = (iota((tok, slots), 1) % cap + 1).astype(f32)
    at_slot = dot_nt(part_of.astype(bf16), of_slot)
    weigh[...] = jnp.where(dot_nt(rank, of_slot) == want, at_slot, 0.0).astype(bf16)

    q_re, q_im = block_diagonal(emi_re[...]), block_diagonal(emi_im[...])

    for i in range(1, n_sp):
        @pl.when(me >= i)
        def _(i=i):
            carry_copy(i).wait_recv()
    run_re = jnp.zeros(mine.shape[1:], f32)
    run_im = run_re
    for i in range(n_sp - 1, 0, -1):
        mul_re, mul_im, add_re, add_im = (pieces[i - 1, plane] for plane in range(4))
        new_re = mul_re * run_re - mul_im * run_im + add_re
        new_im = mul_re * run_im + mul_im * run_re + add_im
        run_re = jnp.where(me >= i, new_re, run_re)
        run_im = jnp.where(me >= i, new_im, run_im)

    for tile in range(tiles):
        at = slice(128 * tile, 128 * tile + 128)
        p_re, p_im, z_re, z_im = ends[tile]
        e_re, e_im = run_re[tile : tile + 1], run_im[tile : tile + 1]
        z_re = z_re + p_re * e_re - p_im * e_im
        z_im = z_im + p_re * e_im + p_im * e_re
        for i in range(n_i):
            step = slice(n_j * i, n_j * i + n_j)
            c_re, c_im = cr[step, at], ci[step, at]
            xr[step, at] = xr[step, at] + c_re * z_re - c_im * z_im
            xi[step, at] = xi[step, at] + c_re * z_im + c_im * z_re
    value = dot_nt(xr[...], q_re, HIGH) - dot_nt(xi[...], q_im, HIGH) + signal * bypass[...]
    order = iota((tok, tok), 1)
    back = where_one((order % n_j) * n_i + order // n_j == iota((tok, tok), 0)).astype(bf16)
    mixed_s[...] = dot(back, jax.nn.gelu(value).astype(bf16)).astype(bf16)

    for i in range(12, 15):
        fetch(i).wait()

    def projected_part(block):
        return dot(mixed_s[...], w[:, cols(block)])

    pair = {}
    for i in range(n_y - 1, -1, -1):
        psend_a[i] = projected_part(y_at(i) * 2 + 1 - core).astype(bf16)
        pair[i] = go(remote(psend_a.at[i], precv_a.at[i], pa_s.at[i], pa_r.at[i], partner))
    across = {}
    for i in range(n_y - 1, 0, -1):
        part = projected_part(y_at(i) * 2 + core)
        pair[i].wait_recv()
        ysend_a[i - 1] = (part + precv_a[i].astype(f32)).astype(bf16)
        across[i] = go(
            remote(
                ysend_a.at[i - 1], yrecv_a.at[i - 1], ya_s.at[i - 1], ya_r.at[i - 1], across_y(i)
            )
        )
    total = projected_part(lane)
    pair[0].wait_recv()
    total = total + precv_a[0].astype(f32)
    for i in range(1, n_y):
        across[i].wait_recv()
        total = total + yrecv_a[i - 1].astype(f32)
    stream = (skip[...].astype(f32) + total.astype(bf16).astype(f32)).astype(bf16)
    stream_s[...] = stream
    stream_f = stream.astype(f32)
    square = jnp.sum(stream_f * stream_f, axis=1, keepdims=True)
    as_rows = jnp.broadcast_to(square, (tok, 128)).T[0:8, :]
    ssend[...] = as_rows
    sums = []
    for i in range(1, n_tp):
        sums.append(
            go(
                remote(
                    ssend, srecv.at[i - 1], sum_s.at[i - 1], sum_r.at[i - 1],
                    (me, lax.rem(lane + i, n_tp)),
                )
            )
        )
    scaled = (stream_f * gain[0:1, cols(lane)]).astype(bf16)

    def put(k):
        return dot(hot[rows_of(k), :], scaled).astype(bf16)

    mine_cols = cols(lane)

    def forward(k):
        here = xs.at[rows_of(k), mine_cols]
        for i in range(1, n_y):
            n = k * (n_y - 1) + i - 1
            go(remote(here, here, f_s.at[n], f_r.at[n], across_y(i)))
        go(remote(here, here, q_s.at[k * n_y], q_r.at[k * n_y], partner))

    def dispatch(k):
        dsend[k - 1] = put(k)
        go(
            remote(
                dsend.at[k - 1], xs.at[rows_of(k), mine_cols], d_s.at[k - 1], d_r.at[k - 1], peer(k)
            )
        )

    first = [n_sp // 2, n_sp // 2 + 1, 1]
    rest = [k for k in list(range(n_sp // 2, n_sp)) + list(range(1, n_sp // 2)) if k not in first]
    for k in first[:1]:
        dispatch(k)
    xs[rows_of(0), mine_cols] = put(0)
    forward(0)
    for k in first[1:]:
        dispatch(k)
    for i, copy in enumerate(sums):
        copy.wait_recv()
        as_rows = as_rows + srecv[i]
    inv = lax.rsqrt(as_rows / width + EPS)
    high = inv.astype(bf16)
    low = (inv - high.astype(f32)).astype(bf16)
    by_slot = dot_nt(high, hot[...]) + dot_nt(low, hot[...])
    part_lane = iota((8, GROUP), 1) // cap
    for k in range(n_sp):
        at = slice(k // per_group * GROUP, k // per_group * GROUP + GROUP)
        scale = jnp.where(part_lane == k % per_group, by_slot[:, at], 0.0)
        if k == 0:
            nrecv[0] = scale
        else:
            nsend[k - 1] = scale
            go(remote(nsend.at[k - 1], nrecv.at[k], n_s.at[k - 1], n_r.at[k - 1], peer(k)))
    for k in rest:
        dispatch(k)

    def landed(k, block, send, recv):
        here = xs.at[rows_of(k), cols(block)]
        remote(here, here, send, recv, partner).wait_recv()

    def members(m):
        return range(m * per_group, m * per_group + per_group)

    def step_a(m):
        for k in members(m):
            if k > 0:
                landed(k, lane, d_s.at[k - 1], d_r.at[k - 1])
                forward(k)

    def from_y(i):
        return lax.rem(y + n_y - i, n_y)

    def step_b(m):
        for k in members(m):
            for i in range(1, n_y):
                n = k * (n_y - 1) + i - 1
                block = from_y(i) * 2 + core
                landed(k, block, f_s.at[n], f_r.at[n])
                here = xs.at[rows_of(k), cols(block)]
                go(remote(here, here, q_s.at[k * n_y + i], q_r.at[k * n_y + i], partner))

    pairs, acrosses, backs = {}, {}, {}

    def step_c(m):
        for k in members(m):
            for i in range(n_y):
                block = from_y(i) * 2 + 1 - core
                landed(k, block, q_s.at[k * n_y + i], q_r.at[k * n_y + i])
        for k in members(m):
            if k > 0:
                remote(
                    nrecv.at[k], nrecv.at[k], n_s.at[k - 1], n_r.at[k - 1], partner
                ).wait_recv()
            scale = nrecv[k] if k % per_group == 0 else scale + nrecv[k]
        scale = jnp.broadcast_to(scale[0:1, :], (GROUP, GROUP)).T[:, 0:1]
        rows = xs[m * GROUP : m * GROUP + GROUP, :]
        gate = dot(rows, wg[...]) * scale
        hidden = (jax.nn.silu(gate) * (dot(rows, wu[...]) * scale)).astype(bf16)
        order = list(range(1, n_y)) + [0]
        for i in order:
            n = m * n_y + i
            psend[n] = dot(hidden, wd[:, cols(y_at(i) * 2 + 1 - core)]).astype(bf16)
            pairs[n] = go(remote(psend.at[n], precv.at[n], p_s.at[n], p_r.at[n], partner))
        for i in order:
            own[m * n_y + i] = dot(hidden, wd[:, cols(y_at(i) * 2 + core)])

    def step_d(m):
        for i in range(1, n_y):
            n, j = m * n_y + i, m * (n_y - 1) + i - 1
            pairs[n].wait_recv()
            ysend[j] = (own[n] + precv[n].astype(f32)).astype(bf16)
            for k in reversed(members(m)):
                at = pl.ds((k % per_group) * cap, cap)
                s = k * (n_y - 1) + i - 1
                acrosses[k, i] = go(
                    remote(ysend.at[j, at], yrecv.at[j, at], y_s.at[s], y_r.at[s], across_y(i))
                )

    def step_e(m):
        pairs[m * n_y].wait_recv()
        for k in reversed(members(m)):
            at = slice((k % per_group) * cap, (k % per_group) * cap + cap)
            total = own[m * n_y, at] + precv[m * n_y, at].astype(f32)
            for i in range(1, n_y):
                acrosses[k, i].wait_recv()
                total = total + yrecv[m * (n_y - 1) + i - 1, at].astype(f32)
            if k > 0:
                rsend[k - 1] = total.astype(bf16)
                backs[k] = go(
                    remote(
                        rsend.at[k - 1], ret.at[rows_of(k)], r_s.at[k - 1], r_r.at[k - 1], peer(k)
                    )
                )
            else:
                ret[rows_of(0), :] = total.astype(bf16)

    step_a(0)
    step_a(2)
    step_b(0)
    step_a(1)
    step_b(2)
    for i in range(15, 18):
        fetch(i).wait()
    step_c(2)
    step_d(2)
    step_b(1)
    step_c(1)
    step_a(3)
    step_e(2)
    step_d(1)
    step_b(3)
    step_c(3)
    step_e(1)
    step_d(3)
    step_c(0)
    step_d(0)
    step_e(3)
    step_e(0)
    total = stream_s[...].astype(f32)
    for m in [2, 1, 3, 0]:
        for k in members(m):
            if k > 0:
                backs[k].wait_recv()
        at = slice(m * GROUP, m * GROUP + GROUP)
        total = total + dot(weigh[:, at], ret[at, :])
    out[...] = total
    for copy in waits:
        copy.wait_send()
    for i in range(1, n_sp):
        @pl.when(me + i < n_sp)
        def _(i=i):
            carry_copy(i).wait_send()


def layer_call(*args):
    n_sp, n_tp = lax.axis_size("sp"), lax.axis_size("tp")
    n_y = n_tp // 2
    f32, bf16 = jnp.float32, jnp.bfloat16
    tok, width = args[13].shape
    d_local = width // n_tp
    chans = args[0].shape[0]
    groups, p_size = args[1].shape
    states = groups * p_size
    slots = 2 * tok * args[10].shape[0]
    cap = slots // n_sp
    n_groups = slots // GROUP
    more = max(n_y - 1, 1)
    plane = (4, states // 128, 128)
    room = [pltpu.VMEM(a.shape, a.dtype) for a in args]
    room[13] = pltpu.VMEM((tok, d_local), bf16)
    pairs = [n_sp - 1, n_sp - 1, n_y, more, n_tp - 1, n_sp - 1, n_sp * more, n_sp * n_y, n_groups * n_y]
    pairs += [n_sp * more, n_sp - 1]
    return pl.pallas_call(
        layer_kernel,
        out_shape=jax.ShapeDtypeStruct((tok, d_local), f32),
        in_specs=[FAR] * N_IN,
        out_specs=VM,
        scratch_shapes=room
        + [DMA((N_IN,))]
        + [pltpu.VMEM((tok, states), f32)] * 4
        + [
            pltpu.VMEM(plane, f32),
            pltpu.VMEM((n_sp - 1,) + plane, f32),
            pltpu.VMEM((tok, chans), bf16),
            pltpu.VMEM((slots, tok), bf16),
            pltpu.VMEM((tok, slots), bf16),
            pltpu.VMEM((tok, d_local), bf16),
            pltpu.VMEM((n_y, tok, d_local), bf16),
            pltpu.VMEM((n_y, tok, d_local), bf16),
            pltpu.VMEM((more, tok, d_local), bf16),
            pltpu.VMEM((more, tok, d_local), bf16),
            pltpu.VMEM((8, tok), f32),
            pltpu.VMEM((n_tp - 1, 8, tok), f32),
            pltpu.VMEM((slots, width), bf16),
            pltpu.VMEM((n_sp - 1, 8, GROUP), f32),
            pltpu.VMEM((n_sp, 8, GROUP), f32),
            pltpu.VMEM((n_sp - 1, cap, d_local), bf16),
            pltpu.VMEM((n_groups * n_y, GROUP, d_local), bf16),
            pltpu.VMEM((n_groups * n_y, GROUP, d_local), f32),
            pltpu.VMEM((n_groups * n_y, GROUP, d_local), bf16),
            pltpu.VMEM((n_groups * more, GROUP, d_local), bf16),
            pltpu.VMEM((n_groups * more, GROUP, d_local), bf16),
            pltpu.VMEM((n_sp - 1, cap, d_local), bf16),
            pltpu.VMEM((slots, d_local), bf16),
        ]
        + [DMA((n,)) for n in pairs for _ in range(2)],
        compiler_params=pltpu.CompilerParams(
            collective_id=0, has_side_effects=True, vmem_limit_bytes=VMEM_ROOM
        ),
        name="layer",
    )(*args)


def per_device(
    lane_source_signal,
    spectral_damping_part,
    spectral_angular_part,
    interval_exponent,
    entry_matrix_inphase,
    entry_matrix_quadrature,
    emission_inphase,
    emission_quadrature,
    lane_bypass_factor,
    spike_shrink_offset,
    lane_exit_matrix,
    skipline_stream,
    specialist_scaling_vector,
    selected_specialists,
    dispatcher_scores,
    specialist_valve_matrix,
    specialist_widen_matrix,
    specialist_shrink_matrix,
):
    p_size = spectral_damping_part.shape[1]
    total = layer_call(
        lane_source_signal,
        spectral_damping_part,
        spectral_angular_part,
        interval_exponent[None, :],
        jnp.swapaxes(entry_matrix_inphase, 1, 2).reshape(-1, p_size),
        jnp.swapaxes(entry_matrix_quadrature, 1, 2).reshape(-1, p_size),
        emission_inphase.reshape(-1, p_size),
        emission_quadrature.reshape(-1, p_size),
        lane_bypass_factor[None, :],
        spike_shrink_offset,
        selected_specialists.T,
        dispatcher_scores.T,
        lane_exit_matrix,
        skipline_stream,
        specialist_scaling_vector[None, :],
        specialist_valve_matrix[0],
        specialist_widen_matrix[0],
        specialist_shrink_matrix[0],
    )
    return total.astype(jnp.bfloat16)


def solution(mesh):
    placed = (
        P("tp", "sp"),
        P("tp", None),
        P("tp", None),
        P("tp"),
        P("tp", None, None),
        P("tp", None, None),
        P("tp", None, None),
        P("tp", None, None),
        P("tp"),
        P("tp", "sp"),
        P("tp", None),
        P("sp", None),
        P(),
        P("sp", None),
        P("sp", None),
        P("sp", None, "tp"),
        P("sp", None, "tp"),
        P("sp", "tp", None),
    )
    return jax.shard_map(
        per_device, mesh=mesh, in_specs=placed, out_specs=P("sp", "tp"), check_vma=False
    )
```

```python
import jax
import jax.numpy as jnp
from jax import lax
from jax.experimental import pallas as pl
from jax.experimental.pallas import tpu as pltpu
from jax.sharding import PartitionSpec as P

EPS = 1e-06
MESH = pl.DeviceIdType.MESH
VM = pl.BlockSpec(memory_space=pltpu.VMEM)
FAR = pl.BlockSpec(memory_space=pl.ANY)
DMA = pltpu.SemaphoreType.DMA
VMEM_ROOM = 48 * 1024 * 1024
HIGH, HIGHEST = lax.Precision.HIGH, lax.Precision.HIGHEST
GROUP = 128


def remote(src, dst, send, recv, where):
    return pltpu.make_async_remote_copy(
        src_ref=src, dst_ref=dst, send_sem=send, recv_sem=recv, device_id=where, device_id_type=MESH
    )


def places():
    n_sp, n_tp = lax.axis_size("sp"), lax.axis_size("tp")
    return n_sp, n_tp, lax.axis_index("sp"), lax.axis_index("tp")


def xor(a, b, n):
    out, bit = 0, 1
    while bit < n:
        p, q = lax.rem(lax.div(a, bit), 2), (b // bit) % 2
        out = out + bit * (p + q - 2 * p * q)
        bit *= 2
    return out


def dot(a, b, precision=None):
    return jnp.dot(a, b, precision=precision, preferred_element_type=jnp.float32)


def dot_nt(a, b, precision=None):
    return lax.dot_general(
        a, b, (((1,), (1,)), ((), ())), precision=precision, preferred_element_type=jnp.float32
    )


def iota(shape, dim):
    return lax.broadcasted_iota(jnp.int32, shape, dim)


def where_one(mask):
    return jnp.where(mask, 1.0, 0.0)


def expm1_of(x):
    series = jnp.ones_like(x)
    for k in range(11, 1, -1):
        series = 1.0 + x * series * (1.0 / k)
    return jnp.where(jnp.abs(x) < 0.7, x * series, jnp.exp(x) - 1.0)


def affine_pair(earlier, latter):
    mul_re = earlier[0] * latter[0] - earlier[1] * latter[1]
    mul_im = earlier[0] * latter[1] + earlier[1] * latter[0]
    add_re = latter[0] * earlier[2] - latter[1] * earlier[3] + latter[2]
    add_im = latter[0] * earlier[3] + latter[1] * earlier[2] + latter[3]
    return (mul_re, mul_im, add_re, add_im)


N_IN = 18


def layer_kernel(*refs):
    f32, bf16 = jnp.float32, jnp.bfloat16
    far = refs[:N_IN]
    out = refs[N_IN]
    near = refs[N_IN + 1 : 2 * N_IN + 1]
    (
        fetched, xr, xi, cr, ci, mine, pieces, mixed_s, hot, weigh, stream_s,
        psend_a, precv_a, ysend_a, yrecv_a, ssend, srecv,
        xs, nsend, nrecv, dsend, psend, own, precv, ysend, yrecv, rsend, ret,
        carry_s, carry_r, n_s, n_r, pa_s, pa_r, ya_s, ya_r, sum_s, sum_r, d_s, d_r,
        f_s, f_r, q_s, q_r, p_s, p_r, y_s, y_r, r_s, r_r,
    ) = refs[2 * N_IN + 1 :]
    (
        u, damp, ang, log_dt, ent_re, ent_im, emi_re, emi_im, bypass, shrink, sel, scores,
        w, skip, gain, wg, wu, wd,
    ) = near
    n_sp, n_tp, me, lane = places()
    n_y = n_tp // 2
    y, core = lax.div(lane, 2), lax.rem(lane, 2)
    partner = (me, y * 2 + 1 - core)
    tok, d_local = out.shape
    slots, width = xs.shape
    cap = slots // n_sp
    per_group = GROUP // cap
    n_groups = slots // GROUP

    def cols(block):
        return pl.ds(pl.multiple_of(block * d_local, 128), d_local)

    def peer(k):
        return (xor(me, k, n_sp), lane)

    def rows_of(k):
        return slice(k * cap, k * cap + cap)

    def y_at(i):
        return lax.rem(y + i, n_y)

    def across_y(i):
        return (me, y_at(i) * 2 + core)

    barrier = pltpu.get_barrier_semaphore()
    peers = [(me, lax.rem(lane + i, n_tp)) for i in range(1, n_tp)]
    peers += [(lax.rem(me + i, n_sp), lane) for i in range(1, n_sp)]
    for other in peers:
        pl.semaphore_signal(barrier, inc=1, device_id=other, device_id_type=MESH)

    def fetch(i):
        src = far[i]
        if i == 13:
            src = src.at[:, cols(lane)]
        return pltpu.make_async_copy(src, near[i], fetched.at[i])

    for i in range(N_IN):
        fetch(i).start()
    for i in range(12):
        fetch(i).wait()

    waits = []

    def go(copy):
        copy.start()
        waits.append(copy)
        return copy

    groups, p_size = damp.shape
    chans = u.shape[0]
    gs = chans // groups
    states = groups * p_size
    tiles = states // 128
    per = 128 // p_size
    n_j = 8
    n_i = tok // n_j

    def lane_group(rows):
        return iota((rows, 128), 1) // p_size

    def as_row(a):
        wide = jnp.concatenate([a] * per, axis=1)
        parts = []
        for tile in range(tiles):
            row = wide[per * tile : per * tile + 1]
            for k in range(1, per):
                row = jnp.where(lane_group(1) == k, wide[per * tile + k : per * tile + k + 1], row)
            parts.append(row)
        return jnp.concatenate(parts, axis=1)

    def spread_tile(columns, tile):
        value = jnp.broadcast_to(columns[:, per * tile : per * tile + 1], (tok, 128))
        for k in range(1, per):
            other = jnp.broadcast_to(columns[:, per * tile + k : per * tile + k + 1], (tok, 128))
            value = jnp.where(lane_group(tok) == k, other, value)
        return value

    block_mask = iota((chans, states), 1) // p_size == iota((chans, states), 0) // gs

    def block_diagonal(a):
        wide = jnp.concatenate([a] * per, axis=1)
        return jnp.where(block_mask, jnp.concatenate([wide] * tiles, axis=1), 0.0)

    eye = where_one(iota((groups, groups), 0) == iota((groups, groups), 1))
    dt = jnp.exp(jnp.sum(eye * log_dt[...], axis=1, keepdims=True))
    a_re, a_im = damp[...], ang[...]
    log_rate = a_re * dt
    angle = a_im * dt
    cos, sin = jnp.cos(angle), jnp.sin(angle)
    half = jnp.sin(0.5 * angle)
    decay = jnp.exp(log_rate)
    num_re = expm1_of(log_rate) * cos - 2.0 * half * half
    num_im = decay * sin
    denom = a_re * a_re + a_im * a_im
    fac_re = as_row((num_re * a_re + num_im * a_im) / denom)
    fac_im = as_row((num_im * a_re - num_re * a_im) / denom)
    lam_re = as_row(decay * cos)
    lam_im = as_row(decay * sin)

    order = iota((tok, tok), 0)
    perm = where_one((order % n_j) * n_i + order // n_j == iota((tok, tok), 1))
    columns = jnp.exp(dot_nt(perm, shrink[...], HIGHEST))
    signal = dot_nt(perm.astype(bf16), u[...])
    in_re, in_im = block_diagonal(ent_re[...]), block_diagonal(ent_im[...])
    drive_re = dot(signal, fac_re * in_re - fac_im * in_im, HIGH)
    drive_im = dot(signal, fac_re * in_im + fac_im * in_re, HIGH)
    row_j = iota((n_j, 128), 0)
    ends = []
    for tile in range(tiles):
        at = slice(128 * tile, 128 * tile + 128)
        modulus = spread_tile(columns, tile)
        t_re, t_im = modulus * lam_re[:, at], modulus * lam_im[:, at]
        for i in range(n_i):
            step = slice(n_j * i, n_j * i + n_j)
            now = (t_re[step], t_im[step], drive_re[step, at], drive_im[step, at])
            run = now if i == 0 else affine_pair(run, now)
            for ref, value in zip((cr, ci, xr, xi), run):
                ref[step, at] = value
        off = 1
        while off < n_j:
            before = [pltpu.roll(value, off, 0) for value in run]
            joined = affine_pair(before, run)
            run = tuple(jnp.where(row_j >= off, new, old) for new, old in zip(joined, run))
            off *= 2
        for plane in range(4):
            mine[plane, tile : tile + 1, :] = run[plane][n_j - 1 : n_j]
        fills = (1.0, 0.0, 0.0, 0.0)
        ends.append(
            [jnp.where(row_j >= 1, pltpu.roll(v, 1, 0), fill) for v, fill in zip(run, fills)]
        )

    pl.semaphore_wait(barrier, len(peers))

    def carry_copy(i):
        return remote(
            mine, pieces.at[i - 1], carry_s.at[i - 1], carry_r.at[i - 1],
            (lax.rem(me + i, n_sp), lane),
        )

    for i in range(1, n_sp):
        @pl.when(me + i < n_sp)
        def _(i=i):
            carry_copy(i).start()

    top = sel.shape[0]
    eye_t = where_one(iota((tok, tok), 0) == iota((tok, tok), 1))
    chosen = dot_nt(eye_t.astype(bf16), sel[...].astype(f32).astype(bf16))
    share = dot_nt(eye_t, scores[...] / jnp.sum(scores[...], axis=0, keepdims=True), HIGHEST)
    index = iota((1, GROUP), 1)
    expert = jnp.where(index < n_sp, xor(me, index, n_sp), -1).astype(f32)
    choice = [chosen[:, k : k + 1] == expert for k in range(top)]
    member = where_one(choice[0])
    part_of = jnp.where(choice[0], share[:, 0:1], 0.0)
    for k in range(1, top):
        member = jnp.where(choice[k], 1.0, member)
        part_of = jnp.where(choice[k], share[:, k : k + 1], part_of)
    below = where_one(iota((tok, tok), 1) <= iota((tok, tok), 0)).astype(bf16)
    rank = (dot(below, member.astype(bf16)) * member).astype(bf16)
    of_slot = where_one(iota((slots, GROUP), 0) // cap == iota((slots, GROUP), 1)).astype(bf16)
    want = (iota((slots, tok), 0) % cap + 1).astype(f32)
    hot[...] = where_one(dot_nt(of_slot, rank) == want).astype(bf16)
    want = (iota((tok, slots), 1) % cap + 1).astype(f32)
    at_slot = dot_nt(part_of.astype(bf16), of_slot)
    weigh[...] = jnp.where(dot_nt(rank, of_slot) == want, at_slot, 0.0).astype(bf16)

    q_re, q_im = block_diagonal(emi_re[...]), block_diagonal(emi_im[...])

    for i in range(1, n_sp):
        @pl.when(me >= i)
        def _(i=i):
            carry_copy(i).wait_recv()
    run_re = jnp.zeros(mine.shape[1:], f32)
    run_im = run_re
    for i in range(n_sp - 1, 0, -1):
        mul_re, mul_im, add_re, add_im = (pieces[i - 1, plane] for plane in range(4))
        new_re = mul_re * run_re - mul_im * run_im + add_re
        new_im = mul_re * run_im + mul_im * run_re + add_im
        run_re = jnp.where(me >= i, new_re, run_re)
        run_im = jnp.where(me >= i, new_im, run_im)

    for tile in range(tiles):
        at = slice(128 * tile, 128 * tile + 128)
        p_re, p_im, z_re, z_im = ends[tile]
        e_re, e_im = run_re[tile : tile + 1], run_im[tile : tile + 1]
        z_re = z_re + p_re * e_re - p_im * e_im
        z_im = z_im + p_re * e_im + p_im * e_re
        for i in range(n_i):
            step = slice(n_j * i, n_j * i + n_j)
            c_re, c_im = cr[step, at], ci[step, at]
            xr[step, at] = xr[step, at] + c_re * z_re - c_im * z_im
            xi[step, at] = xi[step, at] + c_re * z_im + c_im * z_re
    value = dot_nt(xr[...], q_re, HIGH) - dot_nt(xi[...], q_im, HIGH) + signal * bypass[...]
    order = iota((tok, tok), 1)
    back = where_one((order % n_j) * n_i + order // n_j == iota((tok, tok), 0)).astype(bf16)
    mixed_s[...] = dot(back, jax.nn.gelu(value).astype(bf16)).astype(bf16)

    for i in range(12, 15):
        fetch(i).wait()

    def projected_part(block):
        return dot(mixed_s[...], w[:, cols(block)])

    pair = {}
    for i in range(n_y - 1, -1, -1):
        psend_a[i] = projected_part(y_at(i) * 2 + 1 - core).astype(bf16)
        pair[i] = go(remote(psend_a.at[i], precv_a.at[i], pa_s.at[i], pa_r.at[i], partner))
    across = {}
    for i in range(n_y - 1, 0, -1):
        part = projected_part(y_at(i) * 2 + core)
        pair[i].wait_recv()
        ysend_a[i - 1] = (part + precv_a[i].astype(f32)).astype(bf16)
        across[i] = go(
            remote(
                ysend_a.at[i - 1], yrecv_a.at[i - 1], ya_s.at[i - 1], ya_r.at[i - 1], across_y(i)
            )
        )
    total = projected_part(lane)
    pair[0].wait_recv()
    total = total + precv_a[0].astype(f32)
    for i in range(1, n_y):
        across[i].wait_recv()
        total = total + yrecv_a[i - 1].astype(f32)
    stream = (skip[...].astype(f32) + total.astype(bf16).astype(f32)).astype(bf16)
    stream_s[...] = stream
    stream_f = stream.astype(f32)
    square = jnp.sum(stream_f * stream_f, axis=1, keepdims=True)
    as_rows = jnp.broadcast_to(square, (tok, 128)).T[0:8, :]
    ssend[...] = as_rows
    sums = []
    for i in range(1, n_tp):
        sums.append(
            go(
                remote(
                    ssend, srecv.at[i - 1], sum_s.at[i - 1], sum_r.at[i - 1],
                    (me, lax.rem(lane + i, n_tp)),
                )
            )
        )
    scaled = (stream_f * gain[0:1, cols(lane)]).astype(bf16)

    def put(k):
        return dot(hot[rows_of(k), :], scaled).astype(bf16)

    mine_cols = cols(lane)

    def forward(k):
        here = xs.at[rows_of(k), mine_cols]
        for i in range(1, n_y):
            n = k * (n_y - 1) + i - 1
            go(remote(here, here, f_s.at[n], f_r.at[n], across_y(i)))
        go(remote(here, here, q_s.at[k * n_y], q_r.at[k * n_y], partner))

    def dispatch(k):
        dsend[k - 1] = put(k)
        go(
            remote(
                dsend.at[k - 1], xs.at[rows_of(k), mine_cols], d_s.at[k - 1], d_r.at[k - 1], peer(k)
            )
        )

    first = [n_sp // 2, n_sp // 2 + 1, 1]
    rest = [k for k in list(range(2, n_sp)) if k not in first]
    for k in first[:1]:
        dispatch(k)
    xs[rows_of(0), mine_cols] = put(0)
    forward(0)
    for k in first[1:]:
        dispatch(k)
    for i, copy in enumerate(sums):
        copy.wait_recv()
        as_rows = as_rows + srecv[i]
    inv = lax.rsqrt(as_rows / width + EPS)
    high = inv.astype(bf16)
    low = (inv - high.astype(f32)).astype(bf16)
    by_slot = dot_nt(high, hot[...]) + dot_nt(low, hot[...])
    part_lane = iota((8, GROUP), 1) // cap
    for k in range(n_sp):
        at = slice(k // per_group * GROUP, k // per_group * GROUP + GROUP)
        scale = jnp.where(part_lane == k % per_group, by_slot[:, at], 0.0)
        if k == 0:
            nrecv[0] = scale
        else:
            nsend[k - 1] = scale
            go(remote(nsend.at[k - 1], nrecv.at[k], n_s.at[k - 1], n_r.at[k - 1], peer(k)))
    for k in rest:
        dispatch(k)

    def landed(k, block, send, recv):
        here = xs.at[rows_of(k), cols(block)]
        remote(here, here, send, recv, partner).wait_recv()

    def members(m):
        return range(m * per_group, m * per_group + per_group)

    def step_a(m):
        for k in members(m):
            if k > 0:
                landed(k, lane, d_s.at[k - 1], d_r.at[k - 1])
                forward(k)

    def from_y(i):
        return lax.rem(y + n_y - i, n_y)

    def step_b(m):
        for k in members(m):
            for i in range(1, n_y):
                n = k * (n_y - 1) + i - 1
                block = from_y(i) * 2 + core
                landed(k, block, f_s.at[n], f_r.at[n])
                here = xs.at[rows_of(k), cols(block)]
                go(remote(here, here, q_s.at[k * n_y + i], q_r.at[k * n_y + i], partner))

    pairs, acrosses, backs = {}, {}, {}

    def step_c(m):
        for k in members(m):
            for i in range(n_y):
                block = from_y(i) * 2 + 1 - core
                landed(k, block, q_s.at[k * n_y + i], q_r.at[k * n_y + i])
        for k in members(m):
            if k > 0:
                remote(
                    nrecv.at[k], nrecv.at[k], n_s.at[k - 1], n_r.at[k - 1], partner
                ).wait_recv()
            scale = nrecv[k] if k % per_group == 0 else scale + nrecv[k]
        scale = jnp.broadcast_to(scale[0:1, :], (GROUP, GROUP)).T[:, 0:1]
        rows = xs[m * GROUP : m * GROUP + GROUP, :]
        gate = dot(rows, wg[...]) * scale
        hidden = (jax.nn.silu(gate) * (dot(rows, wu[...]) * scale)).astype(bf16)
        order = list(range(1, n_y)) + [0]
        for i in order:
            n = m * n_y + i
            psend[n] = dot(hidden, wd[:, cols(y_at(i) * 2 + 1 - core)]).astype(bf16)
            pairs[n] = go(remote(psend.at[n], precv.at[n], p_s.at[n], p_r.at[n], partner))
        for i in order:
            own[m * n_y + i] = dot(hidden, wd[:, cols(y_at(i) * 2 + core)])

    def step_d(m):
        for i in range(1, n_y):
            n, j = m * n_y + i, m * (n_y - 1) + i - 1
            pairs[n].wait_recv()
            ysend[j] = (own[n] + precv[n].astype(f32)).astype(bf16)
            for k in reversed(members(m)):
                at = pl.ds((k % per_group) * cap, cap)
                s = k * (n_y - 1) + i - 1
                acrosses[k, i] = go(
                    remote(ysend.at[j, at], yrecv.at[j, at], y_s.at[s], y_r.at[s], across_y(i))
                )

    def step_e(m):
        pairs[m * n_y].wait_recv()
        for k in reversed(members(m)):
            at = slice((k % per_group) * cap, (k % per_group) * cap + cap)
            total = own[m * n_y, at] + precv[m * n_y, at].astype(f32)
            for i in range(1, n_y):
                acrosses[k, i].wait_recv()
                total = total + yrecv[m * (n_y - 1) + i - 1, at].astype(f32)
            if k > 0:
                rsend[k - 1] = total.astype(bf16)
                backs[k] = go(
                    remote(
                        rsend.at[k - 1], ret.at[rows_of(k)], r_s.at[k - 1], r_r.at[k - 1], peer(k)
                    )
                )
            else:
                ret[rows_of(0), :] = total.astype(bf16)

    step_a(0)
    step_a(2)
    step_b(0)
    step_a(1)
    for i in range(15, 18):
        fetch(i).wait()
    step_c(0)
    step_b(2)
    step_c(2)
    step_d(2)
    step_b(1)
    step_c(1)
    step_a(3)
    step_e(2)
    step_d(1)
    step_b(3)
    step_c(3)
    step_e(1)
    step_d(3)
    step_d(0)
    step_e(3)
    step_e(0)
    total = stream_s[...].astype(f32)
    for m in [2, 1, 3, 0]:
        for k in members(m):
            if k > 0:
                backs[k].wait_recv()
        at = slice(m * GROUP, m * GROUP + GROUP)
        total = total + dot(weigh[:, at], ret[at, :])
    out[...] = total
    for copy in waits:
        copy.wait_send()
    for i in range(1, n_sp):
        @pl.when(me + i < n_sp)
        def _(i=i):
            carry_copy(i).wait_send()


def layer_call(*args):
    n_sp, n_tp = lax.axis_size("sp"), lax.axis_size("tp")
    n_y = n_tp // 2
    f32, bf16 = jnp.float32, jnp.bfloat16
    tok, width = args[13].shape
    d_local = width // n_tp
    chans = args[0].shape[0]
    groups, p_size = args[1].shape
    states = groups * p_size
    slots = 2 * tok * args[10].shape[0]
    cap = slots // n_sp
    n_groups = slots // GROUP
    more = max(n_y - 1, 1)
    plane = (4, states // 128, 128)
    room = [pltpu.VMEM(a.shape, a.dtype) for a in args]
    room[13] = pltpu.VMEM((tok, d_local), bf16)
    pairs = [n_sp - 1, n_sp - 1, n_y, more, n_tp - 1, n_sp - 1, n_sp * more, n_sp * n_y, n_groups * n_y]
    pairs += [n_sp * more, n_sp - 1]
    return pl.pallas_call(
        layer_kernel,
        out_shape=jax.ShapeDtypeStruct((tok, d_local), f32),
        in_specs=[FAR] * N_IN,
        out_specs=VM,
        scratch_shapes=room
        + [DMA((N_IN,))]
        + [pltpu.VMEM((tok, states), f32)] * 4
        + [
            pltpu.VMEM(plane, f32),
            pltpu.VMEM((n_sp - 1,) + plane, f32),
            pltpu.VMEM((tok, chans), bf16),
            pltpu.VMEM((slots, tok), bf16),
            pltpu.VMEM((tok, slots), bf16),
            pltpu.VMEM((tok, d_local), bf16),
            pltpu.VMEM((n_y, tok, d_local), bf16),
            pltpu.VMEM((n_y, tok, d_local), bf16),
            pltpu.VMEM((more, tok, d_local), bf16),
            pltpu.VMEM((more, tok, d_local), bf16),
            pltpu.VMEM((8, tok), f32),
            pltpu.VMEM((n_tp - 1, 8, tok), f32),
            pltpu.VMEM((slots, width), bf16),
            pltpu.VMEM((n_sp - 1, 8, GROUP), f32),
            pltpu.VMEM((n_sp, 8, GROUP), f32),
            pltpu.VMEM((n_sp - 1, cap, d_local), bf16),
            pltpu.VMEM((n_groups * n_y, GROUP, d_local), bf16),
            pltpu.VMEM((n_groups * n_y, GROUP, d_local), f32),
            pltpu.VMEM((n_groups * n_y, GROUP, d_local), bf16),
            pltpu.VMEM((n_groups * more, GROUP, d_local), bf16),
            pltpu.VMEM((n_groups * more, GROUP, d_local), bf16),
            pltpu.VMEM((n_sp - 1, cap, d_local), bf16),
            pltpu.VMEM((slots, d_local), bf16),
        ]
        + [DMA((n,)) for n in pairs for _ in range(2)],
        compiler_params=pltpu.CompilerParams(
            collective_id=0, has_side_effects=True, vmem_limit_bytes=VMEM_ROOM
        ),
        name="layer",
    )(*[pltpu.with_memory_space_constraint(a, pltpu.HBM) for a in args])


def per_device(
    lane_source_signal,
    spectral_damping_part,
    spectral_angular_part,
    interval_exponent,
    entry_matrix_inphase,
    entry_matrix_quadrature,
    emission_inphase,
    emission_quadrature,
    lane_bypass_factor,
    spike_shrink_offset,
    lane_exit_matrix,
    skipline_stream,
    specialist_scaling_vector,
    selected_specialists,
    dispatcher_scores,
    specialist_valve_matrix,
    specialist_widen_matrix,
    specialist_shrink_matrix,
):
    p_size = spectral_damping_part.shape[1]
    total = layer_call(
        lane_source_signal,
        spectral_damping_part,
        spectral_angular_part,
        interval_exponent[None, :],
        jnp.swapaxes(entry_matrix_inphase, 1, 2).reshape(-1, p_size),
        jnp.swapaxes(entry_matrix_quadrature, 1, 2).reshape(-1, p_size),
        emission_inphase.reshape(-1, p_size),
        emission_quadrature.reshape(-1, p_size),
        lane_bypass_factor[None, :],
        spike_shrink_offset,
        selected_specialists.T,
        dispatcher_scores.T,
        lane_exit_matrix,
        skipline_stream,
        specialist_scaling_vector[None, :],
        specialist_valve_matrix[0],
        specialist_widen_matrix[0],
        specialist_shrink_matrix[0],
    )
    return total.astype(jnp.bfloat16)


def solution(mesh):
    placed = (
        P("tp", "sp"),
        P("tp", None),
        P("tp", None),
        P("tp"),
        P("tp", None, None),
        P("tp", None, None),
        P("tp", None, None),
        P("tp", None, None),
        P("tp"),
        P("tp", "sp"),
        P("tp", None),
        P("sp", None),
        P(),
        P("sp", None),
        P("sp", None),
        P("sp", None, "tp"),
        P("sp", None, "tp"),
        P("sp", "tp", None),
    )
    return jax.shard_map(
        per_device, mesh=mesh, in_specs=placed, out_specs=P("sp", "tp"), check_vma=False
    )
```

```python
import jax
import jax.numpy as jnp
from jax import lax
from jax.experimental import pallas as pl
from jax.experimental.pallas import tpu as pltpu
from jax.sharding import PartitionSpec as P

EPS = 1e-06
MESH = pl.DeviceIdType.MESH
VM = pl.BlockSpec(memory_space=pltpu.VMEM)
FAR = pl.BlockSpec(memory_space=pl.ANY)
DMA = pltpu.SemaphoreType.DMA
VMEM_ROOM = 48 * 1024 * 1024
HIGH, HIGHEST = lax.Precision.HIGH, lax.Precision.HIGHEST
GROUP = 128


def remote(src, dst, send, recv, where):
    return pltpu.make_async_remote_copy(
        src_ref=src, dst_ref=dst, send_sem=send, recv_sem=recv, device_id=where, device_id_type=MESH
    )


def places():
    n_sp, n_tp = lax.axis_size("sp"), lax.axis_size("tp")
    return n_sp, n_tp, lax.axis_index("sp"), lax.axis_index("tp")


def xor(a, b, n):
    out, bit = 0, 1
    while bit < n:
        p, q = lax.rem(lax.div(a, bit), 2), (b // bit) % 2
        out = out + bit * (p + q - 2 * p * q)
        bit *= 2
    return out


def dot(a, b, precision=None):
    return jnp.dot(a, b, precision=precision, preferred_element_type=jnp.float32)


def dot_nt(a, b, precision=None):
    return lax.dot_general(
        a, b, (((1,), (1,)), ((), ())), precision=precision, preferred_element_type=jnp.float32
    )


def iota(shape, dim):
    return lax.broadcasted_iota(jnp.int32, shape, dim)


def where_one(mask):
    return jnp.where(mask, 1.0, 0.0)


def expm1_of(x):
    series = jnp.ones_like(x)
    for k in range(11, 1, -1):
        series = 1.0 + x * series * (1.0 / k)
    return jnp.where(jnp.abs(x) < 0.7, x * series, jnp.exp(x) - 1.0)


def affine_pair(earlier, latter):
    mul_re = earlier[0] * latter[0] - earlier[1] * latter[1]
    mul_im = earlier[0] * latter[1] + earlier[1] * latter[0]
    add_re = latter[0] * earlier[2] - latter[1] * earlier[3] + latter[2]
    add_im = latter[0] * earlier[3] + latter[1] * earlier[2] + latter[3]
    return (mul_re, mul_im, add_re, add_im)


N_IN = 18


def layer_kernel(*refs):
    f32, bf16 = jnp.float32, jnp.bfloat16
    far = refs[:N_IN]
    out = refs[N_IN]
    near = refs[N_IN + 1 : 2 * N_IN + 1]
    (
        fetched, xr, xi, cr, ci, mine, pieces, mixed_s, hot, weigh, stream_s,
        psend_a, precv_a, ysend_a, yrecv_a, ssend, srecv,
        xs, nsend, nrecv, dsend, psend, own, precv, ysend, yrecv, rsend, ret,
        carry_s, carry_r, n_s, n_r, pa_s, pa_r, ya_s, ya_r, sum_s, sum_r, d_s, d_r,
        f_s, f_r, q_s, q_r, p_s, p_r, y_s, y_r, r_s, r_r,
    ) = refs[2 * N_IN + 1 :]
    (
        u, damp, ang, log_dt, ent_re, ent_im, emi_re, emi_im, bypass, shrink, sel, scores,
        w, skip, gain, wg, wu, wd,
    ) = near
    n_sp, n_tp, me, lane = places()
    n_y = n_tp // 2
    y, core = lax.div(lane, 2), lax.rem(lane, 2)
    partner = (me, y * 2 + 1 - core)
    tok, d_local = out.shape
    slots, width = xs.shape
    cap = slots // n_sp
    per_group = GROUP // cap
    n_groups = slots // GROUP

    def cols(block):
        return pl.ds(pl.multiple_of(block * d_local, 128), d_local)

    def peer(k):
        return (xor(me, k, n_sp), lane)

    def rows_of(k):
        return slice(k * cap, k * cap + cap)

    def y_at(i):
        return lax.rem(y + i, n_y)

    def across_y(i):
        return (me, y_at(i) * 2 + core)

    barrier = pltpu.get_barrier_semaphore()
    peers = [(me, lax.rem(lane + i, n_tp)) for i in range(1, n_tp)]
    peers += [(lax.rem(me + i, n_sp), lane) for i in range(1, n_sp)]
    for other in peers:
        pl.semaphore_signal(barrier, inc=1, device_id=other, device_id_type=MESH)

    def fetch(i):
        src = far[i]
        if i == 13:
            src = src.at[:, cols(lane)]
        return pltpu.make_async_copy(src, near[i], fetched.at[i])

    for i in range(N_IN):
        fetch(i).start()
    for i in range(12):
        fetch(i).wait()

    waits = []

    def go(copy):
        copy.start()
        waits.append(copy)
        return copy

    groups, p_size = damp.shape
    chans = u.shape[0]
    gs = chans // groups
    states = groups * p_size
    tiles = states // 128
    per = 128 // p_size
    n_j = 8
    n_i = tok // n_j

    def lane_group(rows):
        return iota((rows, 128), 1) // p_size

    def as_row(a):
        wide = jnp.concatenate([a] * per, axis=1)
        parts = []
        for tile in range(tiles):
            row = wide[per * tile : per * tile + 1]
            for k in range(1, per):
                row = jnp.where(lane_group(1) == k, wide[per * tile + k : per * tile + k + 1], row)
            parts.append(row)
        return jnp.concatenate(parts, axis=1)

    def spread_tile(columns, tile):
        value = jnp.broadcast_to(columns[:, per * tile : per * tile + 1], (tok, 128))
        for k in range(1, per):
            other = jnp.broadcast_to(columns[:, per * tile + k : per * tile + k + 1], (tok, 128))
            value = jnp.where(lane_group(tok) == k, other, value)
        return value

    block_mask = iota((chans, states), 1) // p_size == iota((chans, states), 0) // gs

    def block_diagonal(a):
        wide = jnp.concatenate([a] * per, axis=1)
        return jnp.where(block_mask, jnp.concatenate([wide] * tiles, axis=1), 0.0)

    eye = where_one(iota((groups, groups), 0) == iota((groups, groups), 1))
    dt = jnp.exp(jnp.sum(eye * log_dt[...], axis=1, keepdims=True))
    a_re, a_im = damp[...], ang[...]
    log_rate = a_re * dt
    angle = a_im * dt
    cos, sin = jnp.cos(angle), jnp.sin(angle)
    half = jnp.sin(0.5 * angle)
    decay = jnp.exp(log_rate)
    num_re = expm1_of(log_rate) * cos - 2.0 * half * half
    num_im = decay * sin
    denom = a_re * a_re + a_im * a_im
    fac_re = as_row((num_re * a_re + num_im * a_im) / denom)
    fac_im = as_row((num_im * a_re - num_re * a_im) / denom)
    lam_re = as_row(decay * cos)
    lam_im = as_row(decay * sin)

    order = iota((tok, tok), 0)
    perm = where_one((order % n_j) * n_i + order // n_j == iota((tok, tok), 1))
    columns = jnp.exp(dot_nt(perm, shrink[...], HIGHEST))
    signal = dot_nt(perm.astype(bf16), u[...])
    in_re, in_im = block_diagonal(ent_re[...]), block_diagonal(ent_im[...])
    drive_re = dot(signal, fac_re * in_re - fac_im * in_im, HIGH)
    drive_im = dot(signal, fac_re * in_im + fac_im * in_re, HIGH)
    row_j = iota((n_j, 128), 0)
    ends = []
    for tile in range(tiles):
        at = slice(128 * tile, 128 * tile + 128)
        modulus = spread_tile(columns, tile)
        t_re, t_im = modulus * lam_re[:, at], modulus * lam_im[:, at]
        for i in range(n_i):
            step = slice(n_j * i, n_j * i + n_j)
            now = (t_re[step], t_im[step], drive_re[step, at], drive_im[step, at])
            run = now if i == 0 else affine_pair(run, now)
            for ref, value in zip((cr, ci, xr, xi), run):
                ref[step, at] = value
        off = 1
        while off < n_j:
            before = [pltpu.roll(value, off, 0) for value in run]
            joined = affine_pair(before, run)
            run = tuple(jnp.where(row_j >= off, new, old) for new, old in zip(joined, run))
            off *= 2
        for plane in range(4):
            mine[plane, tile : tile + 1, :] = run[plane][n_j - 1 : n_j]
        fills = (1.0, 0.0, 0.0, 0.0)
        ends.append(
            [jnp.where(row_j >= 1, pltpu.roll(v, 1, 0), fill) for v, fill in zip(run, fills)]
        )

    pl.semaphore_wait(barrier, len(peers))

    def carry_copy(i):
        return remote(
            mine, pieces.at[i - 1], carry_s.at[i - 1], carry_r.at[i - 1],
            (lax.rem(me + i, n_sp), lane),
        )

    for i in range(1, n_sp):
        @pl.when(me + i < n_sp)
        def _(i=i):
            carry_copy(i).start()

    top = sel.shape[0]
    eye_t = where_one(iota((tok, tok), 0) == iota((tok, tok), 1))
    chosen = dot_nt(eye_t.astype(bf16), sel[...].astype(f32).astype(bf16))
    share = dot_nt(eye_t, scores[...] / jnp.sum(scores[...], axis=0, keepdims=True), HIGHEST)
    index = iota((1, GROUP), 1)
    expert = jnp.where(index < n_sp, xor(me, index, n_sp), -1).astype(f32)
    choice = [chosen[:, k : k + 1] == expert for k in range(top)]
    member = where_one(choice[0])
    part_of = jnp.where(choice[0], share[:, 0:1], 0.0)
    for k in range(1, top):
        member = jnp.where(choice[k], 1.0, member)
        part_of = jnp.where(choice[k], share[:, k : k + 1], part_of)
    below = where_one(iota((tok, tok), 1) <= iota((tok, tok), 0)).astype(bf16)
    rank = (dot(below, member.astype(bf16)) * member).astype(bf16)
    of_slot = where_one(iota((slots, GROUP), 0) // cap == iota((slots, GROUP), 1)).astype(bf16)
    want = (iota((slots, tok), 0) % cap + 1).astype(f32)
    hot[...] = where_one(dot_nt(of_slot, rank) == want).astype(bf16)
    want = (iota((tok, slots), 1) % cap + 1).astype(f32)
    at_slot = dot_nt(part_of.astype(bf16), of_slot)
    weigh[...] = jnp.where(dot_nt(rank, of_slot) == want, at_slot, 0.0).astype(bf16)

    q_re, q_im = block_diagonal(emi_re[...]), block_diagonal(emi_im[...])

    for i in range(1, n_sp):
        @pl.when(me >= i)
        def _(i=i):
            carry_copy(i).wait_recv()
    run_re = jnp.zeros(mine.shape[1:], f32)
    run_im = run_re
    for i in range(n_sp - 1, 0, -1):
        mul_re, mul_im, add_re, add_im = (pieces[i - 1, plane] for plane in range(4))
        new_re = mul_re * run_re - mul_im * run_im + add_re
        new_im = mul_re * run_im + mul_im * run_re + add_im
        run_re = jnp.where(me >= i, new_re, run_re)
        run_im = jnp.where(me >= i, new_im, run_im)

    for tile in range(tiles):
        at = slice(128 * tile, 128 * tile + 128)
        p_re, p_im, z_re, z_im = ends[tile]
        e_re, e_im = run_re[tile : tile + 1], run_im[tile : tile + 1]
        z_re = z_re + p_re * e_re - p_im * e_im
        z_im = z_im + p_re * e_im + p_im * e_re
        for i in range(n_i):
            step = slice(n_j * i, n_j * i + n_j)
            c_re, c_im = cr[step, at], ci[step, at]
            xr[step, at] = xr[step, at] + c_re * z_re - c_im * z_im
            xi[step, at] = xi[step, at] + c_re * z_im + c_im * z_re
    value = dot_nt(xr[...], q_re, HIGH) - dot_nt(xi[...], q_im, HIGH) + signal * bypass[...]
    order = iota((tok, tok), 1)
    back = where_one((order % n_j) * n_i + order // n_j == iota((tok, tok), 0)).astype(bf16)
    mixed_s[...] = dot(back, jax.nn.gelu(value).astype(bf16)).astype(bf16)

    for i in range(12, 15):
        fetch(i).wait()

    def projected_part(block):
        return dot(mixed_s[...], w[:, cols(block)])

    pair = {}
    for i in range(n_y - 1, -1, -1):
        psend_a[i] = projected_part(y_at(i) * 2 + 1 - core).astype(bf16)
        pair[i] = go(remote(psend_a.at[i], precv_a.at[i], pa_s.at[i], pa_r.at[i], partner))
    across = {}
    for i in range(n_y - 1, 0, -1):
        part = projected_part(y_at(i) * 2 + core)
        pair[i].wait_recv()
        ysend_a[i - 1] = (part + precv_a[i].astype(f32)).astype(bf16)
        across[i] = go(
            remote(
                ysend_a.at[i - 1], yrecv_a.at[i - 1], ya_s.at[i - 1], ya_r.at[i - 1], across_y(i)
            )
        )
    total = projected_part(lane)
    pair[0].wait_recv()
    total = total + precv_a[0].astype(f32)
    for i in range(1, n_y):
        across[i].wait_recv()
        total = total + yrecv_a[i - 1].astype(f32)
    stream = (skip[...].astype(f32) + total.astype(bf16).astype(f32)).astype(bf16)
    stream_s[...] = stream
    stream_f = stream.astype(f32)
    square = jnp.sum(stream_f * stream_f, axis=1, keepdims=True)
    as_rows = jnp.broadcast_to(square, (tok, 128)).T[0:8, :]
    ssend[...] = as_rows
    sums = []
    for i in range(1, n_tp):
        sums.append(
            go(
                remote(
                    ssend, srecv.at[i - 1], sum_s.at[i - 1], sum_r.at[i - 1],
                    (me, lax.rem(lane + i, n_tp)),
                )
            )
        )
    scaled = (stream_f * gain[0:1, cols(lane)]).astype(bf16)

    def put(k):
        return dot(hot[rows_of(k), :], scaled).astype(bf16)

    mine_cols = cols(lane)

    def forward(k):
        here = xs.at[rows_of(k), mine_cols]
        for i in range(1, n_y):
            n = k * (n_y - 1) + i - 1
            go(remote(here, here, f_s.at[n], f_r.at[n], across_y(i)))
        go(remote(here, here, q_s.at[k * n_y], q_r.at[k * n_y], partner))

    def dispatch(k):
        dsend[k - 1] = put(k)
        go(
            remote(
                dsend.at[k - 1], xs.at[rows_of(k), mine_cols], d_s.at[k - 1], d_r.at[k - 1], peer(k)
            )
        )

    first = list(dict.fromkeys([n_sp // 2, 2, n_sp // 2 + 1, 1]))
    rest = [k for k in list(range(2, n_sp)) if k not in first]
    for k in first[:1]:
        dispatch(k)
    xs[rows_of(0), mine_cols] = put(0)
    forward(0)
    for k in first[1:]:
        dispatch(k)
    for i, copy in enumerate(sums):
        copy.wait_recv()
        as_rows = as_rows + srecv[i]
    inv = lax.rsqrt(as_rows / width + EPS)
    high = inv.astype(bf16)
    low = (inv - high.astype(f32)).astype(bf16)
    by_slot = dot_nt(high, hot[...]) + dot_nt(low, hot[...])
    part_lane = iota((8, GROUP), 1) // cap
    for k in range(n_sp):
        at = slice(k // per_group * GROUP, k // per_group * GROUP + GROUP)
        scale = jnp.where(part_lane == k % per_group, by_slot[:, at], 0.0)
        if k == 0:
            nrecv[0] = scale
        else:
            nsend[k - 1] = scale
            go(remote(nsend.at[k - 1], nrecv.at[k], n_s.at[k - 1], n_r.at[k - 1], peer(k)))
    for k in rest:
        dispatch(k)

    def landed(k, block, send, recv):
        here = xs.at[rows_of(k), cols(block)]
        remote(here, here, send, recv, partner).wait_recv()

    def members(m):
        return range(m * per_group, m * per_group + per_group)

    def step_a(m):
        for k in members(m):
            if k > 0:
                landed(k, lane, d_s.at[k - 1], d_r.at[k - 1])
                forward(k)

    def from_y(i):
        return lax.rem(y + n_y - i, n_y)

    def step_b(m):
        for k in members(m):
            for i in range(1, n_y):
                n = k * (n_y - 1) + i - 1
                block = from_y(i) * 2 + core
                landed(k, block, f_s.at[n], f_r.at[n])
                here = xs.at[rows_of(k), cols(block)]
                go(remote(here, here, q_s.at[k * n_y + i], q_r.at[k * n_y + i], partner))

    pairs, acrosses, backs = {}, {}, {}

    def step_c(m):
        for k in members(m):
            for i in range(n_y):
                block = from_y(i) * 2 + 1 - core
                landed(k, block, q_s.at[k * n_y + i], q_r.at[k * n_y + i])
        for k in members(m):
            if k > 0:
                remote(
                    nrecv.at[k], nrecv.at[k], n_s.at[k - 1], n_r.at[k - 1], partner
                ).wait_recv()
            scale = nrecv[k] if k % per_group == 0 else scale + nrecv[k]
        scale = jnp.broadcast_to(scale[0:1, :], (GROUP, GROUP)).T[:, 0:1]
        rows = xs[m * GROUP : m * GROUP + GROUP, :]
        gate = dot(rows, wg[...]) * scale
        hidden = (jax.nn.silu(gate) * (dot(rows, wu[...]) * scale)).astype(bf16)
        order = list(range(1, n_y)) + [0]
        for i in order:
            n = m * n_y + i
            psend[n] = dot(hidden, wd[:, cols(y_at(i) * 2 + 1 - core)]).astype(bf16)
            pairs[n] = go(remote(psend.at[n], precv.at[n], p_s.at[n], p_r.at[n], partner))
        for i in order:
            own[m * n_y + i] = dot(hidden, wd[:, cols(y_at(i) * 2 + core)])

    def step_d(m):
        for i in range(1, n_y):
            n, j = m * n_y + i, m * (n_y - 1) + i - 1
            pairs[n].wait_recv()
            ysend[j] = (own[n] + precv[n].astype(f32)).astype(bf16)
            for k in reversed(members(m)):
                at = pl.ds((k % per_group) * cap, cap)
                s = k * (n_y - 1) + i - 1
                acrosses[k, i] = go(
                    remote(ysend.at[j, at], yrecv.at[j, at], y_s.at[s], y_r.at[s], across_y(i))
                )

    def step_e(m):
        pairs[m * n_y].wait_recv()
        for k in reversed(members(m)):
            at = slice((k % per_group) * cap, (k % per_group) * cap + cap)
            total = own[m * n_y, at] + precv[m * n_y, at].astype(f32)
            for i in range(1, n_y):
                acrosses[k, i].wait_recv()
                total = total + yrecv[m * (n_y - 1) + i - 1, at].astype(f32)
            if k > 0:
                rsend[k - 1] = total.astype(bf16)
                backs[k] = go(
                    remote(
                        rsend.at[k - 1], ret.at[rows_of(k)], r_s.at[k - 1], r_r.at[k - 1], peer(k)
                    )
                )
            else:
                ret[rows_of(0), :] = total.astype(bf16)

    step_a(0)
    step_a(2)
    step_b(0)
    step_a(1)
    for i in range(15, 18):
        fetch(i).wait()
    step_c(0)
    step_b(2)
    step_c(2)
    step_d(2)
    step_b(1)
    step_c(1)
    step_a(3)
    step_e(2)
    step_d(1)
    step_b(3)
    step_c(3)
    step_e(1)
    step_d(3)
    step_d(0)
    step_e(3)
    step_e(0)
    total = stream_s[...].astype(f32)
    for m in [2, 1, 3, 0]:
        for k in members(m):
            if k > 0:
                backs[k].wait_recv()
        at = slice(m * GROUP, m * GROUP + GROUP)
        total = total + dot(weigh[:, at], ret[at, :])
    out[...] = total
    for copy in waits:
        copy.wait_send()
    for i in range(1, n_sp):
        @pl.when(me + i < n_sp)
        def _(i=i):
            carry_copy(i).wait_send()


def layer_call(*args):
    n_sp, n_tp = lax.axis_size("sp"), lax.axis_size("tp")
    n_y = n_tp // 2
    f32, bf16 = jnp.float32, jnp.bfloat16
    tok, width = args[13].shape
    d_local = width // n_tp
    chans = args[0].shape[0]
    groups, p_size = args[1].shape
    states = groups * p_size
    slots = 2 * tok * args[10].shape[0]
    cap = slots // n_sp
    n_groups = slots // GROUP
    more = max(n_y - 1, 1)
    plane = (4, states // 128, 128)
    room = [pltpu.VMEM(a.shape, a.dtype) for a in args]
    room[13] = pltpu.VMEM((tok, d_local), bf16)
    pairs = [n_sp - 1, n_sp - 1, n_y, more, n_tp - 1, n_sp - 1, n_sp * more, n_sp * n_y, n_groups * n_y]
    pairs += [n_sp * more, n_sp - 1]
    return pl.pallas_call(
        layer_kernel,
        out_shape=jax.ShapeDtypeStruct((tok, d_local), f32),
        in_specs=[FAR] * N_IN,
        out_specs=VM,
        scratch_shapes=room
        + [DMA((N_IN,))]
        + [pltpu.VMEM((tok, states), f32)] * 4
        + [
            pltpu.VMEM(plane, f32),
            pltpu.VMEM((n_sp - 1,) + plane, f32),
            pltpu.VMEM((tok, chans), bf16),
            pltpu.VMEM((slots, tok), bf16),
            pltpu.VMEM((tok, slots), bf16),
            pltpu.VMEM((tok, d_local), bf16),
            pltpu.VMEM((n_y, tok, d_local), bf16),
            pltpu.VMEM((n_y, tok, d_local), bf16),
            pltpu.VMEM((more, tok, d_local), bf16),
            pltpu.VMEM((more, tok, d_local), bf16),
            pltpu.VMEM((8, tok), f32),
            pltpu.VMEM((n_tp - 1, 8, tok), f32),
            pltpu.VMEM((slots, width), bf16),
            pltpu.VMEM((n_sp - 1, 8, GROUP), f32),
            pltpu.VMEM((n_sp, 8, GROUP), f32),
            pltpu.VMEM((n_sp - 1, cap, d_local), bf16),
            pltpu.VMEM((n_groups * n_y, GROUP, d_local), bf16),
            pltpu.VMEM((n_groups * n_y, GROUP, d_local), f32),
            pltpu.VMEM((n_groups * n_y, GROUP, d_local), bf16),
            pltpu.VMEM((n_groups * more, GROUP, d_local), bf16),
            pltpu.VMEM((n_groups * more, GROUP, d_local), bf16),
            pltpu.VMEM((n_sp - 1, cap, d_local), bf16),
            pltpu.VMEM((slots, d_local), bf16),
        ]
        + [DMA((n,)) for n in pairs for _ in range(2)],
        compiler_params=pltpu.CompilerParams(
            collective_id=0, has_side_effects=True, vmem_limit_bytes=VMEM_ROOM
        ),
        name="layer",
    )(*[pltpu.with_memory_space_constraint(a, pltpu.HBM) for a in args])


def per_device(
    lane_source_signal,
    spectral_damping_part,
    spectral_angular_part,
    interval_exponent,
    entry_matrix_inphase,
    entry_matrix_quadrature,
    emission_inphase,
    emission_quadrature,
    lane_bypass_factor,
    spike_shrink_offset,
    lane_exit_matrix,
    skipline_stream,
    specialist_scaling_vector,
    selected_specialists,
    dispatcher_scores,
    specialist_valve_matrix,
    specialist_widen_matrix,
    specialist_shrink_matrix,
):
    p_size = spectral_damping_part.shape[1]
    total = layer_call(
        lane_source_signal,
        spectral_damping_part,
        spectral_angular_part,
        interval_exponent[None, :],
        jnp.swapaxes(entry_matrix_inphase, 1, 2).reshape(-1, p_size),
        jnp.swapaxes(entry_matrix_quadrature, 1, 2).reshape(-1, p_size),
        emission_inphase.reshape(-1, p_size),
        emission_quadrature.reshape(-1, p_size),
        lane_bypass_factor[None, :],
        spike_shrink_offset,
        selected_specialists.T,
        dispatcher_scores.T,
        lane_exit_matrix,
        skipline_stream,
        specialist_scaling_vector[None, :],
        specialist_valve_matrix[0],
        specialist_widen_matrix[0],
        specialist_shrink_matrix[0],
    )
    return total.astype(jnp.bfloat16)


def solution(mesh):
    placed = (
        P("tp", "sp"),
        P("tp", None),
        P("tp", None),
        P("tp"),
        P("tp", None, None),
        P("tp", None, None),
        P("tp", None, None),
        P("tp", None, None),
        P("tp"),
        P("tp", "sp"),
        P("tp", None),
        P("sp", None),
        P(),
        P("sp", None),
        P("sp", None),
        P("sp", None, "tp"),
        P("sp", None, "tp"),
        P("sp", "tp", None),
    )
    return jax.shard_map(
        per_device, mesh=mesh, in_specs=placed, out_specs=P("sp", "tp"), check_vma=False
    )
```
